512 devices in a mesh: ep: 32 (over z, x), tp: 16 (over y, core).
Axes of the slice: x: 4, y: 8, z: 8, core: 2. Of those that a mesh axis runs over, the one named last changes fastest.
Arguments:
- mix_input: bfloat16 [12288, 2048], P('ep', 'tp'), may hold values from -6 to 6
- mix_gain: float32 [2048], replicated, may hold values from 0.1 to 1.9
- gate_b_weight: bfloat16 [2048, 2048], P(None, 'tp'), may hold values from -0.125 to 0.125
- gate_c_weight: bfloat16 [2048, 2048], P(None, 'tp'), may hold values from -0.125 to 0.125
- value_weight: bfloat16 [2048, 2048], P(None, 'tp'), may hold values from -0.125 to 0.125
- conv_weight: float32 [3, 2048], P(None, 'tp'), may hold values from -3 to 3
- out_weight: bfloat16 [2048, 2048], P('tp'), may hold values from -0.125 to 0.125
- expert_input: bfloat16 [5120, 2048], P('ep', 'tp'), may hold values from -6 to 6
- expert_gain: float32 [2048], replicated, may hold values from 0.1 to 1.9
- routes: int32 [5120, 2], P('ep'), may hold values from 0 to 31, all different within a row; in each aligned block of 160 rows (0 to 159, 160 to 319, ...) at most 20 rows name the same one
- route_weight: float32 [5120, 2], P('ep'), may hold values from 0.2 to 1
- expert_gate: bfloat16 [32, 2048, 3072], P('ep', None, 'tp'), may hold values from -0.125 to 0.125
- expert_up: bfloat16 [32, 2048, 3072], P('ep', None, 'tp'), may hold values from -0.125 to 0.125
- expert_down: bfloat16 [32, 3072, 2048], P('ep', 'tp'), may hold values from -0.109375 to 0.109375
Outputs:
- mix_output: bfloat16 [12288, 2048], P('ep', 'tp')
- expert_output: bfloat16 [5120, 2048], P('ep', 'tp')
The draws below stay inside these ranges and needn't reach their ends.
Inputs may be any that keep to these rules, and one draw needn't show every extreme that they name: `routes`: the 2 experts of a row differ. Among the rows of one device no expert is named more than 20 times, a bound that some block reaches.
All inputs are finite; a program needn't handle non-finite values.
Results may differ from the reference program's by a relative error of at most 0.019.
Values may be sent and summed in bfloat16 or wider, within the bound.
A program may use at most 64 MiB of HBM per device.

```python
import math
import jax
import jax.numpy as jnp
import numpy as np
from jax import lax

D = 2048
FF = 3072
TOPK = 2
TOK_B = 160
EXPERTS = 32
CAP = 20
TOKENS_A = 12288
TOKENS_B = 5120
N_EP = 32
N_TP = 16


def levels(own_key, dims, split, low, high):
    def one(position, parts):
        draws = jax.random.uniform(jax.random.fold_in(jax.random.fold_in(own_key, 6), position), (parts,), jnp.float32, low / len(split), high / len(split))
        return jnp.repeat(jnp.exp(draws), dims[position] // parts).reshape((-1,) + (1,) * (len(dims) - position - 1))

    factor_of = one(*split[0])
    for cut in split[1:]:
        factor_of = factor_of * one(*cut)
    return factor_of


def shared_out(stream_key, own, number, rows, count, top, bound, slope):
    ranking = jax.random.permutation(stream_key, count)
    packed, common = load_shares(count, rows * top, bound, slope, True), load_shares(count, rows * top, bound, slope, False)
    places = jnp.arange(count)

    def named(tallies, rotation):
        used = int((tallies > 0).sum())
        fixed = max(1, used // 4)
        passed = fixed + (places - fixed + rotation * (used - fixed)) % max(1, count - fixed)
        return jnp.zeros((count,), jnp.int32).at[ranking[jnp.where(places < fixed, places, passed)]].set(jnp.asarray(tallies, jnp.int32))

    tallies = jnp.where(number % 4 == 0, named(packed, number // 4), named(common, number - number // 4 - 1))
    mixed = jax.random.permutation(jax.random.fold_in(own, 3), count)
    donor, receiver = mixed[0:count // 2 * 2:2], mixed[1:count // 2 * 2:2]
    margin = jnp.minimum(tallies[donor] - 1, bound - tallies[receiver]) // 2
    margin = jnp.where((donor == ranking[0]) | (receiver == ranking[0]) | (tallies[receiver] == 0), 0, jnp.maximum(margin, 0))
    passed = jax.random.randint(jax.random.fold_in(own, 4), (count // 2,), 0, 1 << 20) % (margin + 1)
    tallies = tallies.at[donor].add(-passed).at[receiver].add(passed)
    members = jnp.searchsorted(jnp.cumsum(tallies), jnp.arange(rows * top), side="right").astype(jnp.int32)
    listing = members.reshape(top, rows).T
    listing = listing[jax.random.permutation(jax.random.fold_in(own, 1), rows)]
    rotation = jax.random.randint(jax.random.fold_in(own, 2), (rows, 1), 0, top)
    return jnp.take_along_axis(listing, (jnp.arange(top)[None, :] + rotation) % top, axis=1)


def load_shares(number_of, total, bound, slope, full):
    weights = [(1 << 20) // math.isqrt(standing ** slope) + 1 for standing in range(1, number_of + 1)]
    largest = bound if full else min(bound, max(-(-total // number_of), total * weights[0] // sum(weights)))
    least = 1 if total - largest >= number_of - 1 else 0
    counts, rest = [largest] + [least] * (number_of - 1), total - largest - least * (number_of - 1)
    while rest > 0:
        candidates = [i for i in range(1, number_of) if counts[i] < largest] or [i for i in range(1, number_of) if counts[i] < bound]
        mass, left = sum([weights[i] for i in candidates]), rest
        for i in candidates:
            more = min(bound - counts[i], max(1, left * weights[i] // mass), rest)
            counts[i] = counts[i] + more
            rest = rest - more
    return np.array(counts)


def centred(own_key, shape, scale, reach, pieces=(), kind=jnp.bfloat16):
    drawn = scale * jax.random.normal(own_key, shape, jnp.float32)
    if pieces:
        drawn = drawn * levels(own_key, shape, pieces, -0.22, 0.18)
    return jnp.clip(drawn, -reach, reach).astype(kind)


def setup_inputs(seed: int = 0) -> dict:
    splits = jax.random.split(jax.random.key(seed), 15)
    mix_input = centred(splits[0], (TOKENS_A, D), 1.0, 6.0, ((0, 32), (1, 16)))
    mix_gain = jnp.clip(1.0 + 0.18 * jax.random.normal(splits[1], (D,), jnp.float32), 0.1, 1.9)
    gate_b_weight = centred(splits[2], (D, D), D ** -0.5, 0.125, ((1, 16),))
    gate_c_weight = centred(splits[3], (D, D), D ** -0.5, 0.125, ((1, 16),))
    value_weight = centred(splits[4], (D, D), D ** -0.5, 0.125, ((1, 16),))
    conv_weight = centred(splits[5], (3, D), 0.6, 3.0, ((1, 16),), jnp.float32)
    out_weight = centred(splits[6], (D, D), D ** -0.5, 0.125, ((0, 16),))
    expert_input = centred(splits[7], (TOKENS_B, D), 1.0, 6.0, ((0, 32), (1, 16)))
    expert_gain = jnp.clip(1.0 + 0.18 * jax.random.normal(splits[8], (D,), jnp.float32), 0.1, 1.9)
    routes_keys = jax.random.split(jax.random.fold_in(splits[9], 1), TOKENS_B // TOK_B)
    routes_turns = jax.random.permutation(jax.random.fold_in(splits[9], 3), TOKENS_B // TOK_B)
    routes = jax.vmap(lambda own, number: shared_out(jax.random.fold_in(splits[9], 2), own, number, TOK_B, EXPERTS, TOPK, CAP, 1))(routes_keys, routes_turns).reshape((TOKENS_B, TOPK))
    route_weight = jnp.clip(jnp.exp(math.log(1.0) - 1.609438 * jax.random.uniform(splits[10], (TOKENS_B, TOPK), jnp.float32) ** levels(splits[10], (TOKENS_B, TOPK), ((0, 32),), -0.2, 0.2)), 0.2, 1.0)
    expert_gate = centred(splits[11], (EXPERTS, D, FF), D ** -0.5, 0.125, ((0, 32), (2, 16)))
    expert_up = centred(splits[12], (EXPERTS, D, FF), D ** -0.5, 0.125, ((0, 32), (2, 16)))
    expert_down = centred(splits[13], (EXPERTS, FF, D), FF ** -0.5, 0.109375, ((0, 32), (1, 16)))
    return {"mix_input": mix_input, "mix_gain": mix_gain, "gate_b_weight": gate_b_weight, "gate_c_weight": gate_c_weight, "value_weight": value_weight, "conv_weight": conv_weight, "out_weight": out_weight, "expert_input": expert_input, "expert_gain": expert_gain, "routes": routes, "route_weight": route_weight, "expert_gate": expert_gate, "expert_up": expert_up, "expert_down": expert_down}


epsilon = 1e-06
routed_scale = 2.5

def norm_project(source, gain_vector, matrices):
    widened = source.astype(jnp.float32)
    factor = lax.rsqrt(lax.optimization_barrier(jnp.mean(widened * widened, axis=-1, keepdims=True)) + epsilon)
    scaled = (widened * gain_vector).astype(jnp.bfloat16)
    return [jnp.dot(scaled, matrix, preferred_element_type=jnp.float32) * factor for matrix in matrices]

def block_sum(operand, weights):
    span_size = operand.shape[1] // N_TP
    running = jnp.zeros((operand.shape[0], weights.shape[1]), jnp.float32)
    for block_index in range(N_TP):
        low = block_index * span_size
        partial_value = jnp.dot(operand[:, low:low + span_size], weights[low:low + span_size], preferred_element_type=jnp.float32)
        running = running + partial_value.astype(jnp.bfloat16).astype(jnp.float32)
    return running.astype(jnp.bfloat16)

def reference(mix_input, mix_gain, gate_b_weight, gate_c_weight, value_weight, conv_weight, out_weight, expert_input, expert_gain, routes, route_weight, expert_gate, expert_up, expert_down):
    outer_gate, inner_gate, conv_values = norm_project(mix_input, mix_gain, (gate_b_weight, gate_c_weight, value_weight))
    product = inner_gate * conv_values
    seq_length = product.shape[0]
    padded = jnp.concatenate([jnp.zeros((2, product.shape[1]), jnp.float32), product], axis=0)
    convolved = conv_weight[0] * padded[:seq_length] + conv_weight[1] * padded[1:seq_length + 1] + conv_weight[2] * padded[2:]
    gated = (outer_gate * convolved).astype(jnp.bfloat16)
    mix_output = block_sum(gated, out_weight)
    flat_routes = routes.reshape(-1).astype(jnp.int32)
    pair_count = flat_routes.shape[0]
    slot_count = N_EP * CAP
    expert_ids = jnp.arange(EXPERTS, dtype=jnp.int32)
    matches = (flat_routes[:, None] == expert_ids[None, :]).astype(jnp.int32)
    ranks = lax.optimization_barrier(jnp.sum((jnp.cumsum(matches, axis=0) - matches) * matches, axis=1)).astype(jnp.int32)
    owners_all = (jnp.arange(pair_count, dtype=jnp.int32) // TOPK).astype(jnp.int32)

    def one_expert(inputs):
        gate_matrix, up_matrix, down_matrix, expert_id = inputs
        chosen = flat_routes == expert_id
        target = jnp.where(chosen, ranks, slot_count).astype(jnp.int32)
        owners = jnp.zeros((slot_count,), jnp.int32).at[target].set(owners_all, mode='drop')
        gathered = expert_input[owners]
        hidden_gate, hidden_up = norm_project(gathered, expert_gain, (gate_matrix, up_matrix))
        activated = (jax.nn.silu(hidden_gate) * hidden_up).astype(jnp.bfloat16)
        return block_sum(activated, down_matrix)
    results = lax.map(one_expert, (expert_gate, expert_up, expert_down, expert_ids))
    picked = results[flat_routes, ranks].astype(jnp.float32).reshape(routes.shape[0], TOPK, -1)
    normalized = route_weight / lax.optimization_barrier(jnp.sum(route_weight, axis=1, keepdims=True)) * routed_scale
    expert_output = lax.optimization_barrier(jnp.sum(picked * normalized[:, :, None], axis=1)).astype(jnp.bfloat16)
    return (mix_output, expert_output)
```

```python
import functools

import jax
import jax.numpy as jnp
from jax import lax
from jax.experimental import pallas as pl
from jax.experimental.pallas import tpu as pltpu
from jax.sharding import PartitionSpec as P

epsilon = 1e-06
routed_scale = 2.5
MESH = pl.DeviceIdType.MESH
F32 = jnp.float32
BF16 = jnp.bfloat16
L = 128
W = 2 * L


def mm(a, b):
    return jnp.dot(a, b, preferred_element_type=F32)


def mm_nt(a, b):
    return lax.dot_general(a, b, (((1,), (1,)), ((), ())), preferred_element_type=F32)


def kernel(
    n_ep,
    n_y,
    cap,
    stride,
    mix_in,
    mix_gain,
    gb,
    gc,
    vw,
    cw,
    ow,
    ex_in,
    ex_gain,
    routes,
    scores,
    eg,
    eu,
    ed,
    mix_out,
    ex_out,
    xm,
    xe,
    xsm,
    xse,
    ssm,
    sse,
    wm,
    wo,
    wg,
    wu,
    wd,
    wc,
    rt,
    tpad,
    xpad,
    dsend,
    rbuf,
    prod,
    outer,
    gated,
    act,
    rs_m_send,
    rs_m_recv,
    rs_e_send,
    rs_e_recv,
    ymo,
    ysend,
    rsend,
    ret,
    ag_sem_m,
    ag_sem_e,
    rs_sem_m,
    rs_sem_e,
    d_send,
    d_recv,
    r_send,
    r_recv,
    w_local,
    w_send,
    w_recv,
    misc,
):
    ep = lax.axis_index("ep")
    tp = lax.axis_index("tp")
    y, c = tp // 2, lax.rem(tp, 2)
    o = 1 - c
    partner = 2 * y + o
    half_ep = n_ep // 2
    hs = ep // half_ep
    lm = ep - hs * half_ep
    long, short = n_y // 2, n_y - 1 - n_y // 2
    ring_tp = (2 * lax.rem(y + n_y - 1, n_y) + c, 2 * lax.rem(y + 1, n_y) + c)
    sign = (1, -1)
    rows_m = xm.shape[1]
    rows_e = xe.shape[1]
    hid = wg.shape[0] // 2

    barrier = pltpu.get_barrier_semaphore()

    def greet(j, carry):
        e = lax.rem(ep + j, n_ep)
        pl.semaphore_signal(barrier, inc=1, device_id=(e, 2 * y), device_id_type=MESH)
        pl.semaphore_signal(barrier, inc=1, device_id=(e, 2 * y + 1), device_id_type=MESH)
        return carry

    for t in ring_tp:
        pl.semaphore_signal(barrier, inc=1, device_id=(ep, t), device_id_type=MESH)
    pl.semaphore_signal(barrier, inc=1, device_id=(ep, partner), device_id_type=MESH)
    lax.fori_loop(1, n_ep, greet, 0)

    def lanes(who, base=0):
        return pl.ds(pl.multiple_of(base + who * L, L), L)

    def weight_slots(who):
        return (
            (gb, wm.at[:, lanes(who)]),
            (gc, wm.at[:, lanes(who, W)]),
            (vw, wm.at[:, lanes(who, 2 * W)]),
            (cw, wc.at[who]),
            (ow, wo.at[pl.ds(pl.multiple_of(who * L, L), L)]),
            (eg, wg.at[pl.ds(pl.multiple_of(who * hid, hid), hid)]),
            (eu, wu.at[pl.ds(pl.multiple_of(who * hid, hid), hid)]),
            (ed, wd.at[pl.ds(pl.multiple_of(who * hid, hid), hid)]),
        )

    def mix_half(who):
        return mix_in.at[pl.ds(pl.multiple_of(who * rows_m, rows_m), rows_m)]

    own_mix = pltpu.make_async_copy(mix_half(c), xm.at[y, :, lanes(c)], misc.at[0])
    own_mix.start()
    own_weights = [
        pltpu.make_async_copy(src, dst, w_local.at[i])
        for i, (src, dst) in enumerate(weight_slots(c))
    ]
    for copy in own_weights:
        copy.start()

    tok, top = ex_in.shape[0], routes.shape[0]
    slots_all = n_ep * stride
    rt[...] = jnp.full(rt.shape, -1, jnp.int32)
    rt[0:top, 0:tok] = routes[...]
    tpad[...] = jnp.zeros_like(tpad)
    total_score = scores[0:1, :] + scores[1:2, :]
    tpad[2:3, 0:tok] = scores[0:1, :] / total_score * routed_scale
    tpad[3:4, 0:tok] = scores[1:2, :] / total_score * routed_scale
    xpad[...] = jnp.zeros_like(xpad)
    xpad[0:tok, :] = ex_in[...]
    tokens = rt.shape[1]
    experts = lax.broadcasted_iota(jnp.int32, (n_ep, tokens), 0)
    hit = [experts == rt[k : k + 1, :] for k in range(top)]
    ones = [h.astype(F32) for h in hit]
    before = (
        lax.broadcasted_iota(jnp.int32, (tokens, tokens), 0)
        < lax.broadcasted_iota(jnp.int32, (tokens, tokens), 1)
    ).astype(F32)
    ranks = mm((ones[0] + ones[1]).astype(BF16), before.astype(BF16))
    rows_iota = lax.broadcasted_iota(jnp.int32, (slots_all, tokens), 0)
    table = None
    for k in range(top):
        rank = jnp.sum(ranks * ones[k], axis=0, keepdims=True)
        slot = rt[k : k + 1, :] * stride + rank.astype(jnp.int32)
        tpad[k : k + 1, :] = slot.astype(F32)
        here = rows_iota == slot
        table = here if table is None else table | here
    outgoing = mm(table.astype(F32).astype(BF16), xpad[...]).astype(BF16)
    dsend[...] = outgoing.reshape(dsend.shape)

    pl.semaphore_wait(barrier, 2 * (n_ep - 1) + 3)

    give_mix = pltpu.make_async_remote_copy(
        src_ref=mix_half(o),
        dst_ref=xm.at[y, :, lanes(c)],
        send_sem=misc.at[1],
        recv_sem=misc.at[2],
        device_id=(ep, partner),
        device_id_type=MESH,
    )
    give_mix.start()

    def dispatch_copy(e):
        return pltpu.make_async_remote_copy(
            src_ref=dsend.at[e],
            dst_ref=rbuf.at[c, lm],
            send_sem=d_send.at[e],
            recv_sem=d_recv.at[c * half_ep + lm],
            device_id=(e, 2 * y + hs),
            device_id_type=MESH,
        )

    def dispatch(j, carry):
        dispatch_copy(lax.rem(ep + j, n_ep)).start()
        return carry

    @pl.when(c == hs)
    def _():
        rbuf[c, lm] = dsend[ep]

    @pl.when(c != hs)
    def _():
        dispatch_copy(ep).start()

    lax.fori_loop(1, n_ep, dispatch, 0)

    give_weights = [
        pltpu.make_async_remote_copy(
            src_ref=src,
            dst_ref=dst,
            send_sem=w_send.at[i],
            recv_sem=w_recv.at[i],
            device_id=(ep, partner),
            device_id_type=MESH,
        )
        for i, (src, dst) in enumerate(weight_slots(c))
    ]
    for copy in give_weights:
        copy.start()

    def hops(way, part):
        return long if way == part else short

    def gather_copy(x, sem, way, part, step):
        half = x.shape[1] // 2
        origin = lax.rem(y + sign[way] * step + n_y, n_y)
        block = x.at[origin, pl.ds(part * half, half)]
        return pltpu.make_async_remote_copy(
            src_ref=block,
            dst_ref=block,
            send_sem=sem.at[0, way, part, step],
            recv_sem=sem.at[1, way, part, step],
            device_id=(ep, ring_tp[way]),
            device_id_type=MESH,
        )

    def gather_arrived(x, sem, way, part, step):
        half = x.shape[1] // 2
        origin = lax.rem(y + sign[way] * (step + 1) + n_y, n_y)
        block = x.at[origin, pl.ds(part * half, half)]
        pltpu.make_async_remote_copy(
            src_ref=block,
            dst_ref=block,
            send_sem=sem.at[0, way, part, step],
            recv_sem=sem.at[1, way, part, step],
            device_id=(ep, ring_tp[way]),
            device_id_type=MESH,
        ).wait_recv()

    def gather_start(x, sem):
        for part in range(2):
            for way in range(2):
                if hops(way, part) > 0:
                    gather_copy(x, sem, way, part, 0).start()

    def gather_step(x, sem, step):
        for way in range(2):
            for part in (way, 1 - way):
                if step < hops(way, part):
                    gather_arrived(x, sem, way, part, step)
                    if step + 1 < hops(way, part):
                        gather_copy(x, sem, way, part, step + 1).start()

    def gather_end(x, sem):
        for way in range(2):
            for part in range(2):
                for step in range(hops(way, part)):
                    gather_copy(x, sem, way, part, step).wait_send()

    def scale(x, xs, ss, gain, origin):
        cols = pl.ds(pl.multiple_of(origin * W, W), W)
        wide = x[origin].astype(F32)
        square = wide * wide
        ss[...] += square[:, :L] + square[:, L:]
        xs[:, cols] = (wide * gain[:, cols]).astype(BF16)

    def scale_step(x, xs, ss, gain, step):
        scale(x, xs, ss, gain, lax.rem(y + step + 1, n_y))
        if step < long - 1:
            scale(x, xs, ss, gain, lax.rem(y - step - 1 + n_y, n_y))

    def factor_of(ss):
        return lax.rsqrt(jnp.sum(ss[...], axis=1, keepdims=True) / (n_y * W) + epsilon)

    mix = (xm, ag_sem_m)
    exp = (xe, ag_sem_e)
    mix_scale = (xm, xsm, ssm, mix_gain)
    exp_scale = (xe, xse, sse, ex_gain)

    ssm[...] = jnp.zeros_like(ssm)
    sse[...] = jnp.zeros_like(sse)
    own_mix.wait()
    give_mix.wait_recv()
    gather_start(*mix)
    scale(*mix_scale, y)

    def take_dispatch():
        def one(l, carry):
            for cs in range(2):

                @pl.when(jnp.logical_not((c * half_ep + l == ep) & (c == cs)))
                def _():
                    pltpu.make_async_remote_copy(
                        src_ref=rbuf.at[cs, l],
                        dst_ref=rbuf.at[cs, l],
                        send_sem=d_send.at[l],
                        recv_sem=d_recv.at[cs * half_ep + l],
                        device_id=(ep, partner),
                        device_id_type=MESH,
                    ).wait_recv()

            return carry

        lax.fori_loop(0, half_ep, one, 0)
        wide = half_ep * stride
        row = lax.broadcasted_iota(jnp.int32, (rows_e, wide), 0)
        col = lax.broadcasted_iota(jnp.int32, (rows_e, wide), 1)
        group = (row * (65536 // cap + 1)) >> 16
        pick = (col - row == group * (stride - cap)).astype(F32).astype(BF16)
        for cs in range(2):
            part = rbuf[cs].reshape(wide, L)
            xe[y, :, cs * L : cs * L + L] = mm(pick, part).astype(BF16)
        gather_start(*exp)
        scale(*exp_scale, y)

    def sum_copy(send, recv, sem, way, part, step):
        return pltpu.make_async_remote_copy(
            src_ref=send.at[way, part, step],
            dst_ref=recv.at[way, part, step],
            send_sem=sem.at[0, way, part, step],
            recv_sem=sem.at[1, way, part, step],
            device_id=(ep, ring_tp[way]),
            device_id_type=MESH,
        )

    def partial_sum(left, right, dest, part):
        half = left.shape[0] // 2
        cols = pl.ds(pl.multiple_of(dest * W, W), W)
        return mm(left[part * half : part * half + half], right[:, cols])

    def sum_step(left, right, send, recv, sem, step):
        for way in range(2):
            dest = lax.rem(y - sign[way] * (long - step) + n_y, n_y)
            for part in (way, 1 - way):
                first = long - hops(way, part)
                if step < first:
                    continue
                value = partial_sum(left, right, dest, part)
                if step > first:
                    sum_copy(send, recv, sem, way, part, step - 1).wait_recv()
                    value = value + recv[way, part, step - 1].astype(F32)
                send[way, part, step] = value.astype(BF16)
                sum_copy(send, recv, sem, way, part, step).start()

    def sum_result(left, right, send, recv, sem, part):
        value = partial_sum(left, right, y, part)
        for way in range(2):
            if hops(way, part) > 0:
                sum_copy(send, recv, sem, way, part, long - 1).wait_recv()
                value = value + recv[way, part, long - 1].astype(F32)
        return value.astype(BF16)

    def sum_end(left, right, send, recv, sem):
        for way in range(2):
            for part in range(2):
                for step in range(long - hops(way, part), long):
                    sum_copy(send, recv, sem, way, part, step).wait_send()

    mix_sum = (gated, wo, rs_m_send, rs_m_recv, rs_sem_m)
    exp_sum = (act, wd, rs_e_send, rs_e_recv, rs_sem_e)

    def take_weights(lo, hi):
        for i in range(lo, hi):
            own_weights[i].wait()
            give_weights[i].wait_recv()

    next_ep = jnp.where(c == 0, ep, ep + 1)
    halo = pltpu.make_async_remote_copy(
        src_ref=prod.at[pl.ds(rows_m, 8)],
        dst_ref=prod.at[pl.ds(0, 8)],
        send_sem=misc.at[3],
        recv_sem=misc.at[4],
        device_id=(lax.rem(next_ep, n_ep), partner),
        device_id_type=MESH,
    )
    has_next = jnp.logical_not((c == 1) & (ep == n_ep - 1))
    has_last = jnp.logical_not((c == 0) & (ep == 0))

    def mixer_project():
        factor = factor_of(ssm)
        take_weights(0, 4)
        inner = mm(xsm[...], wm[:, W : 2 * W]) * factor
        values = mm(xsm[...], wm[:, 2 * W :]) * factor
        prod[pl.ds(8, rows_m), :] = inner * values

        @pl.when(has_next)
        def _():
            halo.start()

        outer[...] = mm(xsm[...], wm[:, :W]) * factor

    def mixer_convolve():
        @pl.when(has_last)
        def _():
            halo.wait_recv()

        @pl.when(jnp.logical_not(has_last))
        def _():
            prod[0:8, :] = jnp.zeros((8, W), F32)

        for part in range(2):
            cols = slice(part * L, part * L + L)
            convolved = (
                wc[part, 0:1] * prod[pl.ds(6, rows_m), cols]
                + wc[part, 1:2] * prod[pl.ds(7, rows_m), cols]
                + wc[part, 2:3] * prod[pl.ds(8, rows_m), cols]
            )
            gated[:, cols] = (outer[:, cols] * convolved).astype(BF16)
        take_weights(4, 5)

    def expert_hidden():
        factor = factor_of(sse)
        take_weights(5, 8)
        gate = mm_nt(xse[...], wg[...]) * factor
        up = mm_nt(xse[...], wu[...]) * factor
        act[...] = (gate / (1.0 + jnp.exp(-gate)) * up).astype(BF16)

    give_out = pltpu.make_async_remote_copy(
        src_ref=ysend,
        dst_ref=ymo.at[pl.ds(pl.multiple_of(c * rows_m, rows_m), rows_m)],
        send_sem=misc.at[5],
        recv_sem=misc.at[6],
        device_id=(ep, partner),
        device_id_type=MESH,
    )

    def mixer_result():
        half = rows_m // 2
        for part in range(2):
            value = sum_result(*mix_sum, part)
            left, right = value[:, :L], value[:, L:]
            mine = jnp.where(c == 0, left, right)
            theirs = jnp.where(c == 0, right, left)
            ymo[pl.ds(pl.multiple_of(c * rows_m + part * half, half), half), :] = mine
            ysend[part * half : part * half + half] = theirs
        give_out.start()

    def return_copy(l, cs):
        return pltpu.make_async_remote_copy(
            src_ref=rsend.at[cs, l],
            dst_ref=ret.at[ep],
            send_sem=r_send.at[cs * half_ep + l],
            recv_sem=r_recv.at[ep],
            device_id=(c * half_ep + l, 2 * y + cs),
            device_id_type=MESH,
        )

    def is_self(l, cs):
        return (c * half_ep + l == ep) & (c == cs)

    def return_part(part):
        value = sum_result(*exp_sum, part)
        groups = half_ep // 2
        slots = groups * stride
        row = lax.broadcasted_iota(jnp.int32, (slots, rows_e // 2), 0)
        col = lax.broadcasted_iota(jnp.int32, (slots, rows_e // 2), 1)
        group = (col * (65536 // cap + 1)) >> 16
        pick = (row - col == group * (stride - cap)).astype(F32).astype(BF16)
        spread = mm(pick, value).astype(BF16)
        for cs in range(2):
            piece = spread[:, cs * L : cs * L + L].reshape(groups, stride, L)
            rsend[cs, part * groups : part * groups + groups] = piece

        def one(i, carry):
            l = part * groups + lax.rem(ep + i, groups)
            for cs in range(2):

                @pl.when(jnp.logical_not(is_self(l, cs)))
                def _():
                    return_copy(l, cs).start()

            return carry

        lax.fori_loop(0, groups, one, 0)

    early = min(2, long)
    for step in range(early):
        gather_step(*mix, step)
        scale_step(*mix_scale, step)
    take_dispatch()
    for step in range(early, long):
        gather_step(*mix, step)
        scale_step(*mix_scale, step)
        gather_step(*exp, step - early)
        scale_step(*exp_scale, step - early)
    mixer_project()
    rest = list(range(long - early, long))
    gather_step(*exp, rest[0])
    scale_step(*exp_scale, rest[0])
    mixer_convolve()
    sum_step(*mix_sum, 0)
    for step in rest[1:]:
        gather_step(*exp, step)
        scale_step(*exp_scale, step)
    if long > 1:
        sum_step(*mix_sum, 1)
    expert_hidden()
    for step in range(long):
        sum_step(*exp_sum, step)
        if step + 2 < long:
            sum_step(*mix_sum, step + 2)
    mixer_result()
    for part in range(2):
        return_part(part)

    @pl.when(c == hs)
    def _():
        ret[ep] = rsend[c, lm]

    give_out.wait_recv()
    out_copy = pltpu.make_async_copy(ymo, mix_out, misc.at[7])
    out_copy.start()

    tcol = jnp.transpose(tpad[...])
    lane = lax.broadcasted_iota(jnp.int32, (tok, slots_all), 1)

    def take_return(e, carry):
        @pl.when(jnp.logical_not((e == ep) & (hs == c)))
        def _():
            pltpu.make_async_remote_copy(
                src_ref=ret.at[e],
                dst_ref=ret.at[e],
                send_sem=r_send.at[e],
                recv_sem=r_recv.at[e],
                device_id=(ep, partner),
                device_id_type=MESH,
            ).wait_recv()

        return carry

    lax.fori_loop(0, n_ep, take_return, 0)
    back = ret[...].reshape(slots_all, L)
    total = None
    for k in range(top):
        pick = (lane == tcol[0:tok, k : k + 1].astype(jnp.int32)).astype(F32).astype(BF16)
        term = mm(pick, back) * tcol[0:tok, 2 + k : 3 + k]
        total = term if total is None else total + term
    ex_out[...] = total.astype(BF16)

    def dispatched(j, carry):
        dispatch_copy(lax.rem(ep + j, n_ep)).wait_send()
        return carry

    lax.fori_loop(1, n_ep, dispatched, 0)

    @pl.when(c != hs)
    def _():
        dispatch_copy(ep).wait_send()

    def returned(l, carry):
        for cs in range(2):

            @pl.when(jnp.logical_not(is_self(l, cs)))
            def _():
                return_copy(l, cs).wait_send()

        return carry

    lax.fori_loop(0, half_ep, returned, 0)
    give_mix.wait_send()
    for copy in give_weights:
        copy.wait_send()

    @pl.when(has_next)
    def _():
        halo.wait_send()

    give_out.wait_send()
    gather_end(*mix)
    gather_end(*exp)
    sum_end(*mix_sum)
    sum_end(*exp_sum)
    out_copy.wait()


def local(
    mix_input,
    mix_gain,
    gate_b_weight,
    gate_c_weight,
    value_weight,
    conv_weight,
    out_weight,
    expert_input,
    expert_gain,
    routes,
    route_weight,
    expert_gate,
    expert_up,
    expert_down,
):
    n_ep, n_tp = lax.axis_size("ep"), lax.axis_size("tp")
    n_y = n_tp // 2
    tok, top = routes.shape
    cap = 2 * tok * top // n_ep
    stride = -(-cap // 8) * 8
    half_ep = n_ep // 2
    rows_m = mix_input.shape[0] // 2
    rows_e = half_ep * cap
    width = mix_gain.shape[0]
    hid = expert_gate.shape[2]
    tokens = -(-tok // L) * L
    long = n_y // 2
    slots_all = n_ep * stride
    dma = pltpu.SemaphoreType.DMA
    any_spec = pl.BlockSpec(memory_space=pl.ANY)
    vmem = pl.BlockSpec(memory_space=pltpu.VMEM)
    scratch = [
        pltpu.VMEM((n_y, rows_m, W), BF16),
        pltpu.VMEM((n_y, rows_e, W), BF16),
        pltpu.VMEM((rows_m, width), BF16),
        pltpu.VMEM((rows_e, width), BF16),
        pltpu.VMEM((rows_m, L), F32),
        pltpu.VMEM((rows_e, L), F32),
        pltpu.VMEM((width, 3 * W), BF16),
        pltpu.VMEM((W, width), BF16),
        pltpu.VMEM((2 * hid, width), BF16),
        pltpu.VMEM((2 * hid, width), BF16),
        pltpu.VMEM((2 * hid, width), BF16),
        pltpu.VMEM((2, 3, L), F32),
        pltpu.VMEM((8, tokens), jnp.int32),
        pltpu.VMEM((8, tokens), F32),
        pltpu.VMEM((tokens, L), BF16),
        pltpu.VMEM((n_ep, stride, L), BF16),
        pltpu.VMEM((2, half_ep, stride, L), BF16),
        pltpu.VMEM((8 + rows_m, W), F32),
        pltpu.VMEM((rows_m, W), F32),
        pltpu.VMEM((rows_m, W), BF16),
        pltpu.VMEM((rows_e, 2 * hid), BF16),
        pltpu.VMEM((2, 2, long, rows_m // 2, W), BF16),
        pltpu.VMEM((2, 2, long, rows_m // 2, W), BF16),
        pltpu.VMEM((2, 2, long, rows_e // 2, W), BF16),
        pltpu.VMEM((2, 2, long, rows_e // 2, W), BF16),
        pltpu.VMEM((2 * rows_m, L), BF16),
        pltpu.VMEM((rows_m, L), BF16),
        pltpu.VMEM((2, half_ep, stride, L), BF16),
        pltpu.VMEM((n_ep, stride, L), BF16),
        dma((2, 2, 2, long)),
        dma((2, 2, 2, long)),
        dma((2, 2, 2, long)),
        dma((2, 2, 2, long)),
        dma((n_ep,)),
        dma((n_ep,)),
        dma((n_ep,)),
        dma((n_ep,)),
        dma((8,)),
        dma((8,)),
        dma((8,)),
        dma((8,)),
    ]
    return pl.pallas_call(
        functools.partial(kernel, n_ep, n_y, cap, stride),
        out_shape=(
            jax.ShapeDtypeStruct(mix_input.shape, BF16),
            jax.ShapeDtypeStruct(expert_input.shape, BF16),
        ),
        in_specs=[
            any_spec,
            vmem,
            any_spec,
            any_spec,
            any_spec,
            any_spec,
            any_spec,
            vmem,
            vmem,
            vmem,
            vmem,
            any_spec,
            any_spec,
            any_spec,
        ],
        out_specs=(any_spec, vmem),
        scratch_shapes=scratch,
        compiler_params=pltpu.CompilerParams(
            collective_id=0, has_side_effects=True, vmem_limit_bytes=56 * 1024 * 1024
        ),
    )(
        mix_input,
        mix_gain.reshape(1, width),
        gate_b_weight,
        gate_c_weight,
        value_weight,
        conv_weight,
        out_weight,
        expert_input,
        expert_gain.reshape(1, width),
        routes.T,
        route_weight.T,
        jnp.swapaxes(expert_gate, 1, 2)[0],
        jnp.swapaxes(expert_up, 1, 2)[0],
        expert_down[0],
    )


def solution(mesh):
    in_specs = (
        P("ep", "tp"),
        P(),
        P(None, "tp"),
        P(None, "tp"),
        P(None, "tp"),
        P(None, "tp"),
        P("tp", None),
        P("ep", "tp"),
        P(),
        P("ep", None),
        P("ep", None),
        P("ep", None, "tp"),
        P("ep", None, "tp"),
        P("ep", "tp", None),
    )
    out_specs = (P("ep", "tp"), P("ep", "tp"))
    return jax.shard_map(local, mesh=mesh, in_specs=in_specs, out_specs=out_specs, check_vma=False)
```

```python
import functools

import jax
import jax.numpy as jnp
from jax import lax
from jax.experimental import pallas as pl
from jax.experimental.pallas import tpu as pltpu
from jax.sharding import PartitionSpec as P

epsilon = 1e-06
routed_scale = 2.5
MESH = pl.DeviceIdType.MESH
F32 = jnp.float32
BF16 = jnp.bfloat16
L = 128
W = 2 * L
PARTS = 4
Z = 2 * PARTS
PLACE = {0: 0, 1: 0, -1: 1, 2: 1, -2: 2, 3: 2, -3: 3, 4: 3}
EVEN, ODD = (0, 2, -2, 4), (1, -1, 3, -3)


def mm(a, b):
    return jnp.dot(a, b, preferred_element_type=F32)


def mm_nt(a, b):
    return lax.dot_general(a, b, (((1,), (1,)), ((), ())), preferred_element_type=F32)


def kernel(
    n_ep,
    n_y,
    cap,
    stride,
    mix_in,
    mix_gain_in,
    gb,
    gc,
    vw,
    cw,
    ow,
    ex_in_in,
    ex_gain_in,
    routes_in,
    scores_in,
    eg,
    eu,
    ed,
    mix_out,
    ex_out,
    mix_gain,
    ex_gain,
    routes,
    scores,
    ex_in,
    ga,
    ua,
    xm,
    xe,
    xsm,
    xse,
    ssm,
    sse,
    wm,
    wo,
    wg,
    wu,
    wd,
    wc,
    rt,
    tpad,
    xpad,
    dsend,
    rbuf,
    prod,
    outer,
    gated,
    act,
    rs_m_send,
    rs_m_recv,
    rs_e_send,
    rs_e_recv,
    ymo,
    ysend,
    rsend,
    ret,
    pre_m,
    pre_e,
    ag_sem_m,
    ag_sem_e,
    rs_sem_m,
    rs_sem_e,
    s_sem,
    d_sem,
    w_local,
    w_send,
    w_recv,
    i_sem,
    misc,
):
    ep = lax.axis_index("ep")
    tp = lax.axis_index("tp")
    y, c = tp // 2, lax.rem(tp, 2)
    o = 1 - c
    partner = 2 * y + o
    half_ep = n_ep // 2
    n_x = n_ep // Z
    z, x_own = ep // n_x, lax.rem(ep, n_x)
    hs = lax.rem(z, 2)
    odd = lax.rem(z + c, 2)
    long, short = n_y // 2, n_y - 1 - n_y // 2
    ring_tp = (2 * lax.rem(y + n_y - 1, n_y) + c, 2 * lax.rem(y + 1, n_y) + c)
    sign = (1, -1)
    rows_m = xm.shape[1]
    rows_e = xe.shape[1]
    hid = wg.shape[0] // 2

    def hops(way, part):
        return long if way == part // (PARTS // 2) else short

    order = [(way, part) for part in range(PARTS) for way in range(2)]
    last_first = [(way, part) for part in reversed(range(PARTS)) for way in range(2)]
    place = {}
    for step in range(long):
        for way, part in order:
            if step < hops(way, part):
                place[way, part, step] = len(place)

    barrier = pltpu.get_barrier_semaphore()

    def along_x(off, body):
        lo = 1 if off == 0 else 0

        def one(j, carry):
            body(lax.rem(z + off + Z, Z) * n_x + lax.rem(x_own + j, n_x))
            return carry

        lax.fori_loop(lo, n_x, one, 0)

    def greet(e):
        pl.semaphore_signal(barrier, inc=1, device_id=(e, 2 * y), device_id_type=MESH)
        pl.semaphore_signal(barrier, inc=1, device_id=(e, 2 * y + 1), device_id_type=MESH)

    for t in ring_tp:
        pl.semaphore_signal(barrier, inc=1, device_id=(ep, t), device_id_type=MESH)
    pl.semaphore_signal(barrier, inc=1, device_id=(ep, partner), device_id_type=MESH)
    for off in sorted(PLACE, key=abs, reverse=True):
        along_x(off, greet)

    small = [
        pltpu.make_async_copy(src, dst, i_sem.at[i])
        for i, (src, dst) in enumerate(
            (
                (routes_in, routes),
                (scores_in, scores),
                (ex_in_in, ex_in),
                (mix_gain_in, mix_gain),
                (ex_gain_in, ex_gain),
            )
        )
    ]
    for copy in small:
        copy.start()
    def lanes(who, base=0):
        return pl.ds(pl.multiple_of(base + who * L, L), L)

    def lane_pieces(src, dst, who, base):
        half = src.shape[0] // 2
        return [
            (src.at[pl.ds(i * half, half)], dst.at[pl.ds(i * half, half), lanes(who, base)])
            for i in range(2)
        ]

    def row_pieces(src, dst, who, count):
        rows = src.shape[0] // count
        return [
            (
                src.at[pl.ds(i * rows, rows)],
                dst.at[pl.ds(pl.multiple_of(who * (rows * count) + i * rows, rows), rows)],
            )
            for i in range(count)
        ]

    def weight_slots(who):
        return (
            (lane_pieces(gb, wm, who, 0), gb, wm.at[:, lanes(who)]),
            (lane_pieces(gc, wm, who, W), gc, wm.at[:, lanes(who)]),
            (lane_pieces(vw, wm, who, 2 * W), vw, wm.at[:, lanes(who)]),
            ([(cw, wc.at[who])], cw, wc.at[who]),
            (row_pieces(eg, wg, who, 3), eg, wg.at[pl.ds(0, hid)]),
            (row_pieces(eu, wu, who, 3), eu, wu.at[pl.ds(0, hid)]),
            (row_pieces(ow, wo, who, 2), ow, wo.at[pl.ds(0, L)]),
            (row_pieces(ed, wd, who, 3), ed, wd.at[pl.ds(0, hid)]),
        )

    def mix_half(who):
        return mix_in.at[pl.ds(pl.multiple_of(who * rows_m, rows_m), rows_m)]

    own_mix = pltpu.make_async_copy(mix_half(c), xm.at[y, :, lanes(c)], misc.at[0])
    own_mix.start()
    for i, (pieces, _, _) in enumerate(weight_slots(c)):
        for src, dst in pieces:
            pltpu.make_async_copy(src, dst, w_local.at[i]).start()

    def weight_whole(i):
        _, src, dst = weight_slots(c)[i]
        return pltpu.make_async_remote_copy(
            src_ref=src,
            dst_ref=dst,
            send_sem=w_send.at[i],
            recv_sem=w_recv.at[i],
            device_id=(ep, partner),
            device_id_type=MESH,
        )

    for copy in small:
        copy.wait()

    tok, top = ex_in.shape[0], routes.shape[0]
    slots_all = n_ep * stride
    rt[...] = jnp.full(rt.shape, -1, jnp.int32)
    rt[0:top, 0:tok] = routes[...]
    tpad[...] = jnp.zeros_like(tpad)
    total_score = scores[0:1, :] + scores[1:2, :]
    tpad[2:3, 0:tok] = scores[0:1, :] / total_score * routed_scale
    tpad[3:4, 0:tok] = scores[1:2, :] / total_score * routed_scale
    xpad[...] = jnp.zeros_like(xpad)
    xpad[0:tok, :] = ex_in[...]
    tokens = rt.shape[1]
    experts = lax.broadcasted_iota(jnp.int32, (n_ep, tokens), 0)
    hit = [experts == rt[k : k + 1, :] for k in range(top)]
    ones = [h.astype(F32) for h in hit]
    before = (
        lax.broadcasted_iota(jnp.int32, (tokens, tokens), 0)
        < lax.broadcasted_iota(jnp.int32, (tokens, tokens), 1)
    ).astype(F32)
    ranks = mm((ones[0] + ones[1]).astype(BF16), before.astype(BF16))
    rows_iota = lax.broadcasted_iota(jnp.int32, (slots_all, tokens), 0)
    table = None
    for k in range(top):
        rank = jnp.sum(ranks * ones[k], axis=0, keepdims=True)
        slot = rt[k : k + 1, :] * stride + rank.astype(jnp.int32)
        tpad[k : k + 1, :] = slot.astype(F32)
        here = rows_iota == slot
        table = here if table is None else table | here
    outgoing = mm(table.astype(F32).astype(BF16), xpad[...]).astype(BF16)
    dsend[...] = outgoing.reshape(dsend.shape)

    pl.semaphore_wait(barrier, 2 * (n_ep - 1) + 3)

    give_mix = pltpu.make_async_remote_copy(
        src_ref=mix_half(o),
        dst_ref=xm.at[y, :, lanes(c)],
        send_sem=misc.at[1],
        recv_sem=misc.at[2],
        device_id=(ep, partner),
        device_id_type=MESH,
    )
    give_mix.start()

    def dispatch_copy(off, e):
        return pltpu.make_async_remote_copy(
            src_ref=dsend.at[e],
            dst_ref=rbuf.at[c, PLACE[off] * n_x + x_own],
            send_sem=s_sem.at[0],
            recv_sem=d_sem.at[PLACE[off]],
            device_id=(e, 2 * y + hs),
            device_id_type=MESH,
        )

    @pl.when(c == hs)
    def _():
        rbuf[c, x_own] = dsend[ep]

    @pl.when(c != hs)
    def _():
        dispatch_copy(0, ep).start()

    for off in sorted(PLACE, key=abs):
        along_x(-off, lambda e: dispatch_copy(off, e).start())

    waiting = [
        (i, src, dst)
        for i, (pieces, _, _) in enumerate(weight_slots(c))
        for src, dst in pieces
    ]

    def feed(count=1):
        for _ in range(min(count, len(waiting))):
            i, src, dst = waiting.pop(0)
            pltpu.make_async_remote_copy(
                src_ref=src,
                dst_ref=dst,
                send_sem=w_send.at[i],
                recv_sem=w_recv.at[i],
                device_id=(ep, partner),
                device_id_type=MESH,
            ).start()

    def gather_block(x, way, part, step):
        rows = x.shape[1] // PARTS
        origin = lax.rem(y + sign[way] * step + n_y, n_y)
        return x.at[origin, pl.ds(part * rows, rows)]

    def gather_copy(x, sem, out, way, part, step):
        block = gather_block(x, way, part, step)
        return pltpu.make_async_remote_copy(
            src_ref=block,
            dst_ref=block,
            send_sem=s_sem.at[out],
            recv_sem=sem.at[place[way, part, step]],
            device_id=(ep, ring_tp[way]),
            device_id_type=MESH,
        )

    def gather_arrived(x, sem, out, way, part, step):
        block = gather_block(x, way, part, step + 1)
        pltpu.make_async_remote_copy(
            src_ref=block,
            dst_ref=block,
            send_sem=s_sem.at[out],
            recv_sem=sem.at[place[way, part, step]],
            device_id=(ep, ring_tp[way]),
            device_id_type=MESH,
        ).wait_recv()

    def gather_start(x, sem, out, parts):
        for part in parts:
            for way in range(2):
                if hops(way, part) > 0:
                    gather_copy(x, sem, out, way, part, 0).start()

    def gather_step(x, sem, out, step, parts=range(PARTS)):
        for way, part in order:
            if part in parts:
                if step < hops(way, part):
                    gather_arrived(x, sem, out, way, part, step)
                    if step + 1 < hops(way, part):
                        gather_copy(x, sem, out, way, part, step + 1).start()
                if way == 1:
                    feed()

    def sent(ref, sem):
        pltpu.make_async_remote_copy(
            src_ref=ref,
            dst_ref=ref,
            send_sem=sem,
            recv_sem=sem,
            device_id=(ep, partner),
            device_id_type=MESH,
        ).wait_send()

    def received(ref, sem):
        pltpu.make_async_remote_copy(
            src_ref=ref,
            dst_ref=ref,
            send_sem=sem,
            recv_sem=sem,
            device_id=(ep, partner),
            device_id_type=MESH,
        ).wait_recv()

    def scale(x, xs, ss, gain, origin):
        cols = pl.ds(pl.multiple_of(origin * W, W), W)
        wide = x[origin].astype(F32)
        square = wide * wide
        ss[...] += square[:, :L] + square[:, L:]
        xs[:, cols] = (wide * gain[:, cols]).astype(BF16)

    def scale_step(x, xs, ss, gain, step):
        scale(x, xs, ss, gain, lax.rem(y + step + 1, n_y))
        if step < long - 1:
            scale(x, xs, ss, gain, lax.rem(y - step - 1 + n_y, n_y))

    def factor_of(ss):
        return lax.rsqrt(jnp.sum(ss[...], axis=1, keepdims=True) / (n_y * W) + epsilon)

    mix = (xm, ag_sem_m, 2)
    exp = (xe, ag_sem_e, 3)
    mix_scale = (xm, xsm, ssm, mix_gain)
    exp_scale = (xe, xse, sse, ex_gain)

    ssm[...] = jnp.zeros_like(ssm)
    sse[...] = jnp.zeros_like(sse)
    own_mix.wait()
    give_mix.wait_recv()
    gather_start(*mix, range(PARTS))
    scale(*mix_scale, y)

    def take_dispatch(part):
        rows, groups = rows_e // PARTS, n_x
        span = pl.ds(part * groups, groups)
        if part == 0:

            @pl.when(c == hs)
            def _():
                received(dsend.at[pl.ds(0, 2 * groups - 1)], d_sem.at[part])

            @pl.when(c != hs)
            def _():
                received(dsend.at[pl.ds(0, 2 * groups)], d_sem.at[part])

        else:
            received(dsend.at[pl.ds(0, 2 * groups)], d_sem.at[part])
        wide = groups * stride
        row = lax.broadcasted_iota(jnp.int32, (rows, wide), 0)
        col = lax.broadcasted_iota(jnp.int32, (rows, wide), 1)
        group = (row * (65536 // cap + 1)) >> 16
        pick = (col - row == group * (stride - cap)).astype(F32).astype(BF16)
        for cs in range(2):
            piece = mm(pick, rbuf[cs, span].reshape(wide, L)).astype(BF16)
            xe[y, part * rows : part * rows + rows, cs * L : cs * L + L] = piece
        gather_start(*exp, (part,))
        if part == PARTS - 1:
            scale(*exp_scale, y)

    def sum_copy(send, recv, sem, out, way, part, step):
        slot = place[way, part, step - (long - hops(way, part))]
        return pltpu.make_async_remote_copy(
            src_ref=send.at[slot],
            dst_ref=recv.at[slot],
            send_sem=s_sem.at[out],
            recv_sem=sem.at[slot],
            device_id=(ep, ring_tp[way]),
            device_id_type=MESH,
        )

    def sum_in(recv, way, part, step):
        return recv[place[way, part, step - (long - hops(way, part))]].astype(F32)

    def prepare(left, right, pre, step):
        half = left.shape[0] // 2
        if step == long:
            cols = pl.ds(pl.multiple_of(y * W, W), W)
            pre[0] = mm(left[...], right[:, cols])
            return
        for way in range(2):
            dest = lax.rem(y - sign[way] * (long - step) + n_y, n_y)
            cols = pl.ds(pl.multiple_of(dest * W, W), W)
            if step < long - short:
                rows = slice(way * half, way * half + half)
                pre[way, rows] = mm(left[rows], right[:, cols])
            else:
                pre[way] = mm(left[...], right[:, cols])

    def sum_step(left, right, pre, send, recv, sem, out, step):
        if step == 0:
            prepare(left, right, pre, 0)
        rows = left.shape[0] // PARTS
        for way, part in last_first:
            first = long - hops(way, part)
            if step < first:
                continue
            value = pre[way, part * rows : part * rows + rows]
            if step > first:
                sum_copy(send, recv, sem, out, way, part, step - 1).wait_recv()
                value = value + sum_in(recv, way, part, step - 1)
            send[place[way, part, step - first]] = value.astype(BF16)
            sum_copy(send, recv, sem, out, way, part, step).start()
        prepare(left, right, pre, step + 1)

    def sum_result(left, right, pre, send, recv, sem, out, part):
        rows = left.shape[0] // PARTS
        value = pre[0, part * rows : part * rows + rows]
        for way in range(2):
            if hops(way, part) > 0:
                sum_copy(send, recv, sem, out, way, part, long - 1).wait_recv()
                value = value + sum_in(recv, way, part, long - 1)
        return value.astype(BF16)

    mix_sum = (gated, wo, pre_m, rs_m_send, rs_m_recv, rs_sem_m, 4)
    exp_sum = (act, wd, pre_e, rs_e_send, rs_e_recv, rs_sem_e, 5)

    def take_weights(lo, hi):
        for i in range(lo, hi):
            _, src, dst = weight_slots(c)[i]
            pltpu.make_async_copy(src, dst, w_local.at[i]).wait()
            weight_whole(i).wait_recv()

    next_ep = jnp.where(c == 0, ep, ep + 1)
    halo = pltpu.make_async_remote_copy(
        src_ref=prod.at[pl.ds(rows_m, 8)],
        dst_ref=prod.at[pl.ds(0, 8)],
        send_sem=misc.at[3],
        recv_sem=misc.at[4],
        device_id=(lax.rem(next_ep, n_ep), partner),
        device_id_type=MESH,
    )
    has_next = jnp.logical_not((c == 1) & (ep == n_ep - 1))
    has_last = jnp.logical_not((c == 0) & (ep == 0))

    def mixer_project():
        factor = factor_of(ssm)
        take_weights(0, 4)
        inner = mm(xsm[...], wm[:, W : 2 * W]) * factor
        values = mm(xsm[...], wm[:, 2 * W :]) * factor
        prod[pl.ds(8, rows_m), :] = inner * values

        @pl.when(has_next)
        def _():
            halo.start()

        outer[...] = mm(xsm[...], wm[:, :W]) * factor

    def mixer_convolve():
        @pl.when(has_last)
        def _():
            halo.wait_recv()

        @pl.when(jnp.logical_not(has_last))
        def _():
            prod[0:8, :] = jnp.zeros((8, W), F32)

        for part in range(2):
            cols = slice(part * L, part * L + L)
            convolved = (
                wc[part, 0:1] * prod[pl.ds(6, rows_m), cols]
                + wc[part, 1:2] * prod[pl.ds(7, rows_m), cols]
                + wc[part, 2:3] * prod[pl.ds(8, rows_m), cols]
            )
            gated[:, cols] = (outer[:, cols] * convolved).astype(BF16)
        take_weights(6, 7)

    def expert_hidden():
        factor = factor_of(sse)
        take_weights(7, 8)
        gate = ga[...] * factor
        up = ua[...] * factor
        act[...] = (gate / (1.0 + jnp.exp(-gate)) * up).astype(BF16)

    def expert_project(step):
        origins = [lax.rem(y + step + 1, n_y)]
        if step < long - 1:
            origins.append(lax.rem(y - step - 1 + n_y, n_y))
        if step == 0:
            origins.append(y)
            take_weights(4, 6)
        for acc, weight in ((ga, wg), (ua, wu)):
            value = None if step == 0 else acc[...]
            for origin in origins:
                cols = pl.ds(pl.multiple_of(origin * W, W), W)
                term = mm_nt(xse[:, cols], weight[:, cols])
                value = term if value is None else value + term
            acc[...] = value

    give_out = pltpu.make_async_remote_copy(
        src_ref=ysend,
        dst_ref=ymo.at[pl.ds(pl.multiple_of(c * rows_m, rows_m), rows_m)],
        send_sem=misc.at[5],
        recv_sem=misc.at[6],
        device_id=(ep, partner),
        device_id_type=MESH,
    )

    def mixer_result():
        half = rows_m // PARTS
        for part in range(PARTS):
            value = sum_result(*mix_sum, part)
            left, right = value[:, :L], value[:, L:]
            mine = jnp.where(c == 0, left, right)
            theirs = jnp.where(c == 0, right, left)
            ymo[pl.ds(pl.multiple_of(c * rows_m + part * half, half), half), :] = mine
            ysend[part * half : part * half + half] = theirs
        give_out.start()

    def return_copy(part, j, cs):
        off = EVEN[part] + odd * (ODD[part] - EVEN[part])
        return pltpu.make_async_remote_copy(
            src_ref=rsend.at[cs, part * n_x + j],
            dst_ref=ret.at[ep],
            send_sem=s_sem.at[6],
            recv_sem=s_sem.at[7],
            device_id=(lax.rem(z + off + Z, Z) * n_x + j, 2 * y + cs),
            device_id_type=MESH,
        )

    def return_part(part):
        value = sum_result(*exp_sum, part)
        groups = n_x
        slots = groups * stride
        row = lax.broadcasted_iota(jnp.int32, (slots, rows_e // PARTS), 0)
        col = lax.broadcasted_iota(jnp.int32, (slots, rows_e // PARTS), 1)
        group = (col * (65536 // cap + 1)) >> 16
        pick = (row - col == group * (stride - cap)).astype(F32).astype(BF16)
        spread = mm(pick, value).astype(BF16)
        for cs in range(2):
            piece = spread[:, cs * L : cs * L + L].reshape(groups, stride, L)
            rsend[cs, part * groups : part * groups + groups] = piece

        def one(i, carry):
            j = lax.rem(x_own + i, n_x)
            for cs in range(2):
                if part == 0:

                    @pl.when(jnp.logical_not((hs == c) & (j == x_own) & (c == cs)))
                    def _():
                        return_copy(part, j, cs).start()

                else:
                    return_copy(part, j, cs).start()
            return carry

        lax.fori_loop(0, groups, one, 0)

    turn = max(1, long - 2)
    gather_step(*mix, 0)
    scale_step(*mix_scale, 0)
    take_dispatch(0)
    if long > 1:
        gather_step(*mix, 1, (0, 1))
        take_dispatch(1)
        gather_step(*mix, 1, (2, 3))
        scale_step(*mix_scale, 1)
    else:
        take_dispatch(1)
    take_dispatch(2)
    if long > 2:
        gather_step(*mix, 2, (0, 1))
        take_dispatch(3)
        gather_step(*mix, 2, (2, 3))
        scale_step(*mix_scale, 2)
    else:
        take_dispatch(3)
    for step in range(3, long):
        for part in range(PARTS):
            gather_step(*exp, step - 3, (part,))
            gather_step(*mix, step, (part,))
        scale_step(*mix_scale, step)
    for step in range(long):
        if step == turn:
            mixer_convolve()
            sum_step(*mix_sum, 0)
        if step >= long - 3 or long < 4:
            gather_step(*exp, step)
        scale_step(*exp_scale, step)
        if step == 0:
            feed(len(waiting))
            mixer_project()
        expert_project(step)
        if step == turn:
            sum_step(*mix_sum, 1)
    if long == 1:
        mixer_convolve()
        sum_step(*mix_sum, 0)
    expert_hidden()
    for step in range(long):
        sum_step(*exp_sum, step)
        if step + 2 < long:
            sum_step(*mix_sum, step + 2)
    mixer_result()
    for part in reversed(range(PARTS)):
        return_part(part)

    @pl.when(c == hs)
    def _():
        ret[ep] = rsend[c, x_own]

    give_out.wait_recv()
    mix_out[...] = ymo[...]

    tcol = jnp.transpose(tpad[...])
    lane = lax.broadcasted_iota(jnp.int32, (tok, slots_all), 1)

    picks = [
        (lane == tcol[0:tok, k : k + 1].astype(jnp.int32)).astype(F32).astype(BF16)
        for k in range(top)
    ]

    @pl.when(c == hs)
    def _():
        sent(dsend.at[pl.ds(0, n_ep - 1)], s_sem.at[0])
        sent(dsend.at[pl.ds(0, n_ep - 1)], s_sem.at[6])

    @pl.when(c != hs)
    def _():
        sent(dsend, s_sem.at[0])
        sent(dsend, s_sem.at[6])

    give_mix.wait_send()
    for i in range(8):
        weight_whole(i).wait_send()

    @pl.when(has_next)
    def _():
        halo.wait_send()

    give_out.wait_send()
    sent(xm.at[pl.ds(0, n_y - 1)], s_sem.at[2])
    sent(xe.at[pl.ds(0, n_y - 1)], s_sem.at[3])
    sent(rs_m_send, s_sem.at[4])
    sent(rs_e_send, s_sem.at[5])

    @pl.when(c == hs)
    def _():
        received(dsend.at[pl.ds(0, n_ep - 1)], s_sem.at[7])

    @pl.when(c != hs)
    def _():
        received(dsend, s_sem.at[7])

    back = ret[...].reshape(slots_all, L)
    total = None
    for k in range(top):
        term = mm(picks[k], back) * tcol[0:tok, 2 + k : 3 + k]
        total = term if total is None else total + term
    ex_out[...] = total.astype(BF16)


def local(
    mix_input,
    mix_gain,
    gate_b_weight,
    gate_c_weight,
    value_weight,
    conv_weight,
    out_weight,
    expert_input,
    expert_gain,
    routes,
    route_weight,
    expert_gate,
    expert_up,
    expert_down,
):
    n_ep, n_tp = lax.axis_size("ep"), lax.axis_size("tp")
    n_y = n_tp // 2
    tok, top = routes.shape
    cap = 2 * tok * top // n_ep
    stride = -(-cap // 8) * 8
    half_ep = n_ep // 2
    rows_m = mix_input.shape[0] // 2
    rows_e = half_ep * cap
    width = mix_gain.shape[0]
    hid = expert_gate.shape[2]
    tokens = -(-tok // L) * L
    long = n_y // 2
    slots_all = n_ep * stride
    dma = pltpu.SemaphoreType.DMA
    any_spec = pl.BlockSpec(memory_space=pl.ANY)
    vmem = pl.BlockSpec(memory_space=pltpu.VMEM)
    scratch = [
        pltpu.VMEM((1, width), F32),
        pltpu.VMEM((1, width), F32),
        pltpu.VMEM((top, tok), jnp.int32),
        pltpu.VMEM((top, tok), F32),
        pltpu.VMEM((tok, L), BF16),
        pltpu.VMEM((rows_e, 2 * hid), F32),
        pltpu.VMEM((rows_e, 2 * hid), F32),
        pltpu.VMEM((n_y, rows_m, W), BF16),
        pltpu.VMEM((n_y, rows_e, W), BF16),
        pltpu.VMEM((rows_m, width), BF16),
        pltpu.VMEM((rows_e, width), BF16),
        pltpu.VMEM((rows_m, L), F32),
        pltpu.VMEM((rows_e, L), F32),
        pltpu.VMEM((width, 3 * W), BF16),
        pltpu.VMEM((W, width), BF16),
        pltpu.VMEM((2 * hid, width), BF16),
        pltpu.VMEM((2 * hid, width), BF16),
        pltpu.VMEM((2 * hid, width), BF16),
        pltpu.VMEM((2, 3, L), F32),
        pltpu.VMEM((8, tokens), jnp.int32),
        pltpu.VMEM((8, tokens), F32),
        pltpu.VMEM((tokens, L), BF16),
        pltpu.VMEM((n_ep, stride, L), BF16),
        pltpu.VMEM((2, half_ep, stride, L), BF16),
        pltpu.VMEM((8 + rows_m, W), F32),
        pltpu.VMEM((rows_m, W), F32),
        pltpu.VMEM((rows_m, W), BF16),
        pltpu.VMEM((rows_e, 2 * hid), BF16),
        pltpu.VMEM((PARTS * (n_y - 1), rows_m // PARTS, W), BF16),
        pltpu.VMEM((PARTS * (n_y - 1), rows_m // PARTS, W), BF16),
        pltpu.VMEM((PARTS * (n_y - 1), rows_e // PARTS, W), BF16),
        pltpu.VMEM((PARTS * (n_y - 1), rows_e // PARTS, W), BF16),
        pltpu.VMEM((2 * rows_m, L), BF16),
        pltpu.VMEM((rows_m, L), BF16),
        pltpu.VMEM((2, half_ep, stride, L), BF16),
        pltpu.VMEM((n_ep, stride, L), BF16),
        pltpu.VMEM((2, rows_m, W), F32),
        pltpu.VMEM((2, rows_e, W), F32),
        dma((PARTS * (n_y - 1),)),
        dma((PARTS * (n_y - 1),)),
        dma((PARTS * (n_y - 1),)),
        dma((PARTS * (n_y - 1),)),
        dma((8,)),
        dma((PARTS,)),
        dma((8,)),
        dma((8,)),
        dma((8,)),
        dma((5,)),
        dma((7,)),
    ]
    return pl.pallas_call(
        functools.partial(kernel, n_ep, n_y, cap, stride),
        out_shape=(
            pltpu.VMEM(mix_input.shape, BF16),
            pltpu.VMEM(expert_input.shape, BF16),
        ),
        in_specs=[any_spec] * 14,
        out_specs=(vmem, vmem),
        scratch_shapes=scratch,
        compiler_params=pltpu.CompilerParams(
            collective_id=0, has_side_effects=True, vmem_limit_bytes=56 * 1024 * 1024
        ),
    )(
        mix_input,
        mix_gain.reshape(1, width),
        gate_b_weight,
        gate_c_weight,
        value_weight,
        conv_weight,
        out_weight,
        expert_input,
        expert_gain.reshape(1, width),
        routes.T,
        route_weight.T,
        jnp.swapaxes(expert_gate, 1, 2)[0],
        jnp.swapaxes(expert_up, 1, 2)[0],
        expert_down[0],
    )


def solution(mesh):
    in_specs = (
        P("ep", "tp"),
        P(),
        P(None, "tp"),
        P(None, "tp"),
        P(None, "tp"),
        P(None, "tp"),
        P("tp", None),
        P("ep", "tp"),
        P(),
        P("ep", None),
        P("ep", None),
        P("ep", None, "tp"),
        P("ep", None, "tp"),
        P("ep", "tp", None),
    )
    out_specs = (P("ep", "tp"), P("ep", "tp"))
    return jax.shard_map(local, mesh=mesh, in_specs=in_specs, out_specs=out_specs, check_vma=False)
```

```python
import functools

import jax
import jax.numpy as jnp
from jax import lax
from jax.experimental import pallas as pl
from jax.experimental.pallas import tpu as pltpu
from jax.sharding import PartitionSpec as P

epsilon = 1e-06
routed_scale = 2.5
MESH = pl.DeviceIdType.MESH
F32 = jnp.float32
BF16 = jnp.bfloat16
L = 128
W = 2 * L
MIX_PARTS = 4
Z = 8
OFFS = (0, 1, -1, 2, -2, 3, -3, 4)


def mm(a, b):
    return jnp.dot(a, b, preferred_element_type=F32)


def mm_nt(a, b):
    return lax.dot_general(a, b, (((1,), (1,)), ((), ())), preferred_element_type=F32)


def kernel(*args):
    for core in range(2):

        @pl.when(lax.rem(lax.axis_index("tp"), 2) == core)
        def _():
            body(core, *args)


def body(
    c,
    n_ep,
    n_y,
    cap,
    stride,
    mix_in,
    mix_gain_in,
    gb,
    gc,
    vw,
    cw,
    ow,
    ex_in_in,
    ex_gain_in,
    routes_in,
    scores_in,
    eg,
    eu,
    ed,
    out,
    gain,
    routes,
    scores,
    ex_in,
    acc_gate,
    acc_up,
    xm,
    xe,
    xsm,
    xse,
    ssm,
    sse,
    wm,
    wo,
    wg,
    wu,
    wd,
    wc,
    rt,
    tpad,
    xpad,
    dsend,
    rbuf,
    prod,
    outer,
    gated,
    act,
    rs_m_send,
    rs_m_recv,
    rs_e_send,
    rs_e_recv,
    ymo,
    rsend,
    ret,
    pre_m,
    pre_e,
    ag_sem,
    rs_sem,
    s_sem,
    d_sem,
    w_local,
    w_send,
    w_recv,
    i_sem,
    misc,
    go,
    acc_mix,
):
    ep = lax.axis_index("ep")
    tp = lax.axis_index("tp")
    y = tp // 2
    partner = 2 * y + 1 - c
    n_x = n_ep // Z
    z, x_own = ep // n_x, lax.rem(ep, n_x)
    long, short = n_y // 2, n_y - 1 - n_y // 2
    ring_tp = (2 * lax.rem(y + n_y - 1, n_y) + c, 2 * lax.rem(y + 1, n_y) + c)
    sign = (1, -1)
    hid = wg.shape[0] // 2
    tok, top = ex_in.shape[0], routes.shape[0]
    rows_m = xm.shape[1]
    x, xs, ss = ((xm, xsm, ssm), (xe, xse, sse))[c]
    send, recv, pre = ((rs_m_send, rs_m_recv, pre_m), (rs_e_send, rs_e_recv, pre_e))[c]
    parts = (MIX_PARTS, Z)[c]
    rows = x.shape[1] // parts

    def hops(way, part):
        return long if way == part % 2 else short

    order = [(way, part) for part in range(parts) for way in range(2)]
    last_first = [(way, part) for part in reversed(range(parts)) for way in range(2)]
    place = {}
    for step in range(long):
        for way, part in order:
            if step < hops(way, part):
                place[way, part, step] = len(place)

    def remote(src, dst, send_sem, recv_sem, device):
        return pltpu.make_async_remote_copy(
            src_ref=src,
            dst_ref=dst,
            send_sem=send_sem,
            recv_sem=recv_sem,
            device_id=device,
            device_id_type=MESH,
        )

    def sent(ref, sem):
        remote(ref, ref, sem, sem, (ep, partner)).wait_send()

    def received(ref, sem):
        remote(ref, ref, sem, sem, (ep, partner)).wait_recv()

    barrier = pltpu.get_barrier_semaphore()

    def along_x(off, act_on):
        def one(j, carry):
            act_on(lax.rem(z + off + Z, Z) * n_x + lax.rem(x_own + j, n_x))
            return carry

        lax.fori_loop(1 if off == 0 else 0, n_x, one, 0)

    small = [
        pltpu.make_async_copy(src, dst, i_sem.at[i])
        for i, (src, dst) in enumerate(
            (
                (routes_in, routes),
                (scores_in, scores),
                (ex_in_in, ex_in),
                ((mix_gain_in, ex_gain_in)[c], gain),
            )
        )
    ]
    for copy in small:
        copy.start()

    def greet(e):
        pl.semaphore_signal(barrier, inc=1, device_id=(e, 2 * y), device_id_type=MESH)
        pl.semaphore_signal(barrier, inc=1, device_id=(e, 2 * y + 1), device_id_type=MESH)

    for off in reversed(OFFS):
        along_x(off, greet)
    for t in ring_tp + (partner,):
        pl.semaphore_signal(barrier, inc=1, device_id=(ep, t), device_id_type=MESH)

    def weight_slots(core, who):
        if core == 0:
            return (
                (gb, wm.at[:, pl.ds(who * L, L)]),
                (gc, wm.at[:, pl.ds(W + who * L, L)]),
                (vw, wm.at[:, pl.ds(2 * W + who * L, L)]),
                (cw, wc.at[who]),
                (ow, wo.at[pl.ds(who * L, L)]),
            )
        return (
            (eg, wg.at[pl.ds(who * hid, hid)]),
            (eu, wu.at[pl.ds(who * hid, hid)]),
            (ed, wd.at[pl.ds(who * hid, hid)]),
        )

    own_weights = [
        pltpu.make_async_copy(src, dst, w_local.at[i])
        for i, (src, dst) in enumerate(weight_slots(c, c))
    ]
    give_weights = [
        remote(src, dst, w_send.at[i], w_recv.at[i], (ep, partner))
        for i, (src, dst) in enumerate(weight_slots(1 - c, c))
    ]
    if c == 0:
        own_mix = pltpu.make_async_copy(mix_in, xm.at[y, :, pl.ds(0, L)], misc.at[0])
        own_mix.start()
    for copy in own_weights:
        copy.start()

    def take_weights(lo, hi):
        for i in range(lo, hi):
            own_weights[i].wait()
            received(weight_slots(c, 1 - c)[i][1], w_recv.at[i])

    for copy in small:
        copy.wait()

    slots_all = n_ep * stride
    rt[...] = jnp.full(rt.shape, -1, jnp.int32)
    rt[0:top, 0:tok] = routes[...]
    tpad[...] = jnp.zeros_like(tpad)
    total_score = scores[0:1, :] + scores[1:2, :]
    tpad[2:3, 0:tok] = scores[0:1, :] / total_score * routed_scale
    tpad[3:4, 0:tok] = scores[1:2, :] / total_score * routed_scale
    xpad[...] = jnp.zeros_like(xpad)
    xpad[0:tok, :] = ex_in[...]
    tokens = rt.shape[1]
    experts = lax.broadcasted_iota(jnp.int32, (n_ep, tokens), 0)
    ones = [(experts == rt[k : k + 1, :]).astype(F32) for k in range(top)]
    before = (
        lax.broadcasted_iota(jnp.int32, (tokens, tokens), 0)
        < lax.broadcasted_iota(jnp.int32, (tokens, tokens), 1)
    ).astype(F32)
    ranks = mm((ones[0] + ones[1]).astype(BF16), before.astype(BF16))
    rows_iota = lax.broadcasted_iota(jnp.int32, (slots_all, tokens), 0)
    table = None
    for k in range(top):
        rank = jnp.sum(ranks * ones[k], axis=0, keepdims=True)
        slot = rt[k : k + 1, :] * stride + rank.astype(jnp.int32)
        tpad[k : k + 1, :] = slot.astype(F32)
        here = rows_iota == slot
        table = here if table is None else table | here
    outgoing = mm(table.astype(F32).astype(BF16), xpad[...]).astype(BF16)
    dsend[...] = outgoing.reshape(dsend.shape)
    ss[...] = jnp.zeros_like(ss)

    pl.semaphore_wait(barrier, 2 * (n_ep - 1) + 3)

    if c == 1:
        give_mix = remote(
            mix_in, xm.at[y, :, pl.ds(L, L)], misc.at[1], misc.at[2], (ep, partner)
        )
        give_mix.start()

    def dispatch_copy(index, e):
        return remote(
            dsend.at[e],
            rbuf.at[c, index * n_x + x_own],
            s_sem.at[0],
            d_sem.at[index],
            (e, 2 * y + 1),
        )

    if c == 1:
        rbuf[1, x_own] = dsend[ep]
    else:
        dispatch_copy(0, ep).start()
    for index, off in enumerate(OFFS):
        along_x(-off, lambda e: dispatch_copy(index, e).start())
    for copy in give_weights:
        copy.start()

    def gather_block(way, part, step):
        origin = lax.rem(y + sign[way] * step + n_y, n_y)
        return x.at[origin, pl.ds(part * rows, rows)]

    def gather_send(way, part, step):
        block = gather_block(way, part, step)
        sem = ag_sem.at[place[way, part, step]]
        remote(block, block, s_sem.at[1], sem, (ep, ring_tp[way])).start()

    def gather_start(part):
        for way in range(2):
            if hops(way, part) > 0:
                gather_send(way, part, 0)

    def gather_step(step, some):
        for way, part in order:
            if part in some and step < hops(way, part):
                received(gather_block(way, part, step + 1), ag_sem.at[place[way, part, step]])
                if step + 1 < hops(way, part):
                    gather_send(way, part, step + 1)

    def scale(origin):
        cols = pl.ds(pl.multiple_of(origin * W, W), W)
        wide = x[origin].astype(F32)
        square = wide * wide
        ss[...] += square[:, :L] + square[:, L:]
        xs[:, cols] = (wide * gain[:, cols]).astype(BF16)

    def origins_of(step):
        found = [lax.rem(y + step + 1, n_y)]
        if step < long - 1:
            found.append(lax.rem(y - step - 1 + n_y, n_y))
        return found

    def scale_step(step):
        for origin in origins_of(step):
            scale(origin)

    def factor_of(lo=0, hi=x.shape[1]):
        return lax.rsqrt(jnp.sum(ss[lo:hi], axis=1, keepdims=True) / (n_y * W) + epsilon)

    left, right = ((gated, wo), (act, wd))[c]

    def sum_slot(way, part, step):
        return place[way, part, step - (long - hops(way, part))]

    def sum_in(way, part, step):
        slot = sum_slot(way, part, step)
        received(recv.at[slot], rs_sem.at[slot])
        return recv[slot].astype(F32)

    def prepare(step, lo=0, hi=x.shape[1]):
        for way in range(2 if 0 < step < long else 1):
            dest = y if step == long else lax.rem(y - sign[way] * (long - step) + n_y, n_y)
            cols = pl.ds(pl.multiple_of(dest * W, W), W)
            pre[way, lo:hi] = mm(left[lo:hi], right[:, cols])

    def sum_sends(step, some):
        for way, part in last_first:
            first = long - hops(way, part)
            if step < first or part not in some:
                continue
            value = pre[way if step > 0 else 0, part * rows : part * rows + rows]
            if step > first:
                value = value + sum_in(way, part, step - 1)
            slot = sum_slot(way, part, step)
            send[slot] = value.astype(BF16)
            remote(
                send.at[slot], recv.at[slot], s_sem.at[2], rs_sem.at[slot], (ep, ring_tp[way])
            ).start()

    def sum_step(step):
        sum_sends(step, range(parts))
        prepare(step + 1)

    def sum_result(part):
        value = pre[0, part * rows : part * rows + rows]
        for way in range(2):
            if hops(way, part) > 0:
                value = value + sum_in(way, part, long - 1)
        return value.astype(BF16)

    def slot_table(shape, row_dim):
        row = lax.broadcasted_iota(jnp.int32, shape, row_dim)
        slot = lax.broadcasted_iota(jnp.int32, shape, 1 - row_dim)
        group = (row * (65536 // cap + 1)) >> 16
        return (slot - row == group * (stride - cap)).astype(F32).astype(BF16)

    if c == 0:
        own_mix.wait()
        received(xm.at[y, :, pl.ds(L, L)], misc.at[2])
        for part in range(parts):
            gather_start(part)
        scale(y)
        for step in range(long):
            gather_step(step, range(parts))
            scale_step(step)
            origins = origins_of(step)
            if step == 0:
                origins.append(y)
                take_weights(0, 4)
            value = None if step == 0 else acc_mix[...]
            for origin in origins:
                cols = pl.ds(pl.multiple_of(origin * W, W), W)
                term = mm(xs[:, cols], wm[cols, :])
                value = term if value is None else value + term
            acc_mix[...] = value

        factor = factor_of()

        def product(lo, hi):
            part = factor[lo:hi]
            inner = acc_mix[lo:hi, W : 2 * W] * part
            prod[8 + lo : 8 + hi, :] = inner * (acc_mix[lo:hi, 2 * W :] * part)

        product(rows_m - 16, rows_m)
        halo = remote(
            prod.at[pl.ds(rows_m, 8)],
            prod.at[pl.ds(0, 8)],
            misc.at[3],
            misc.at[4],
            (lax.rem(ep + 1, n_ep), tp),
        )

        @pl.when(ep < n_ep - 1)
        def _():
            halo.start()

        product(0, rows_m - 16)
        outer[...] = acc_mix[:, :W] * factor

        take_weights(4, 5)

        def convolve(lo, hi):
            for h in range(2):
                cols = slice(h * L, h * L + L)
                convolved = (
                    wc[h, 0:1] * prod[6 + lo : 6 + hi, cols]
                    + wc[h, 1:2] * prod[7 + lo : 7 + hi, cols]
                    + wc[h, 2:3] * prod[8 + lo : 8 + hi, cols]
                )
                gated[lo:hi, cols] = (outer[lo:hi, cols] * convolved).astype(BF16)

        convolve(16, rows_m)
        prepare(0, rows, rows_m)
        sum_sends(0, range(1, parts))

        @pl.when(ep > 0)
        def _():
            halo.wait_recv()

        @pl.when(ep == 0)
        def _():
            prod[0:8, :] = jnp.zeros((8, W), F32)

        convolve(0, 16)
        prepare(0, 0, rows)
        sum_sends(0, (0,))
        prepare(1)
        for step in range(1, long):
            if step == long - 1:
                pl.semaphore_wait(go.at[0], 1)
            sum_step(step)
        if long == 1:
            pl.semaphore_wait(go.at[0], 1)
        give_out = remote(ymo, ymo, misc.at[5], misc.at[6], (ep, partner))
        for part in range(parts):
            value = sum_result(part)
            out[part * rows : part * rows + rows, :] = value[:, :L]
            ymo[part * rows : part * rows + rows, :] = value[:, L:]
        give_out.start()
    else:

        def take_dispatch(part):
            count = 2 * n_x - (1 if part == 0 else 0)
            received(dsend.at[pl.ds(0, count)], d_sem.at[part])
            pick = slot_table((rows, n_x * stride), 0)
            for cs in range(2):
                block = rbuf[cs, pl.ds(part * n_x, n_x)].reshape(n_x * stride, L)
                piece = mm(pick, block).astype(BF16)
                xe[y, part * rows : part * rows + rows, cs * L : cs * L + L] = piece
            gather_start(part)

        def project(step):
            origins = origins_of(step)
            if step == 0:
                origins.append(y)
                take_weights(0, 2)
            for acc, weight in ((acc_gate, wg), (acc_up, wu)):
                value = None if step == 0 else acc[...]
                for origin in origins:
                    cols = pl.ds(pl.multiple_of(origin * W, W), W)
                    term = mm_nt(xs[:, cols], weight[:, cols])
                    value = term if value is None else value + term
                acc[...] = value

        for part in range(parts):
            take_dispatch(part)
            if part >= parts // 2 - 1:
                gather_step(0, (part - parts // 2 + 1,))
        scale(y)
        gather_step(0, range(parts // 2 + 1, parts))
        if long > 1:
            gather_step(1, range(parts))
        scale_step(0)
        project(0)
        for step in range(1, long):
            if step > 1:
                gather_step(step, range(parts))
            scale_step(step)
            project(step)
        take_weights(2, 3)
        half = x.shape[1] // 2
        for lo in (half, 0):
            factor = factor_of(lo, lo + half)
            gate = acc_gate[lo : lo + half] * factor
            up = acc_up[lo : lo + half] * factor
            act[lo : lo + half] = (gate / (1.0 + jnp.exp(-gate)) * up).astype(BF16)
            prepare(0, lo, lo + half)
            sum_sends(0, range(lo // rows, (lo + half) // rows))
        prepare(1)
        for step in range(1, long):
            sum_step(step)

        def return_copy(part, j, cs):
            return remote(
                rsend.at[cs, part * n_x + j],
                ret.at[ep],
                s_sem.at[3 + cs],
                s_sem.at[5],
                (lax.rem(z + OFFS[part] + Z, Z) * n_x + j, 2 * y + cs),
            )

        spread_table = slot_table((n_x * stride, rows), 1)
        for part in reversed(range(parts)):
            spread = mm(spread_table, sum_result(part)).astype(BF16)
            if part == 4:
                pl.semaphore_signal(
                    go.at[0], inc=1, device_id=(ep, partner), device_id_type=MESH
                )
            for cs in range(2):
                piece = spread[:, cs * L : cs * L + L].reshape(n_x, stride, L)
                rsend[cs, part * n_x : part * n_x + n_x] = piece

            def one(i, carry):
                j = lax.rem(x_own + i, n_x)
                return_copy(part, j, 0).start()
                if part > 0:
                    return_copy(part, j, 1).start()
                else:

                    @pl.when(j != x_own)
                    def _():
                        return_copy(part, j, 1).start()

                return carry

            lax.fori_loop(0, n_x, one, 0)
        ret[ep] = rsend[1, x_own]

    tcol = jnp.transpose(tpad[...])
    lane = lax.broadcasted_iota(jnp.int32, (tok, slots_all), 1)
    picks = [
        (lane == tcol[0:tok, k : k + 1].astype(jnp.int32)).astype(F32).astype(BF16)
        for k in range(top)
    ]
    for i in range(len(give_weights)):
        give_weights[i].wait_send()
    sent(dsend.at[pl.ds(0, n_ep - c)], s_sem.at[0])
    sent(x.at[pl.ds(0, n_y - 1)], s_sem.at[1])
    sent(send, s_sem.at[2])
    if c == 0:

        @pl.when(ep < n_ep - 1)
        def _():
            halo.wait_send()

        give_out.wait_send()
    else:
        give_mix.wait_send()
        received(ymo, misc.at[6])
        out[pl.ds(0, rows_m), :] = ymo[...]
        sent(rsend.at[0], s_sem.at[3])
        sent(rsend.at[1, pl.ds(0, n_ep - 1)], s_sem.at[4])
    received(dsend.at[pl.ds(0, n_ep - c)], s_sem.at[5])
    back = ret[...].reshape(slots_all, L)
    total = None
    for k in range(top):
        term = mm(picks[k], back) * tcol[0:tok, 2 + k : 3 + k]
        total = term if total is None else total + term
    out[pl.ds(rows_m, tok), :] = total.astype(BF16)


def local(
    mix_input,
    mix_gain,
    gate_b_weight,
    gate_c_weight,
    value_weight,
    conv_weight,
    out_weight,
    expert_input,
    expert_gain,
    routes,
    route_weight,
    expert_gate,
    expert_up,
    expert_down,
):
    n_ep, n_tp = lax.axis_size("ep"), lax.axis_size("tp")
    n_y = n_tp // 2
    tok, top = routes.shape
    cap = 2 * tok * top // n_ep
    stride = -(-cap // 8) * 8
    rows_m = mix_input.shape[0]
    rows_e = n_ep * cap
    width = mix_gain.shape[0]
    hid = expert_gate.shape[2]
    tokens = -(-tok // L) * L
    mix_slots, ex_slots = MIX_PARTS * (n_y - 1), Z * (n_y - 1)
    dma = pltpu.SemaphoreType.DMA
    any_spec = pl.BlockSpec(memory_space=pl.ANY)
    vmem = pl.BlockSpec(memory_space=pltpu.VMEM)
    scratch = [
        pltpu.VMEM((1, width), F32),
        pltpu.VMEM((top, tok), jnp.int32),
        pltpu.VMEM((top, tok), F32),
        pltpu.VMEM((tok, L), BF16),
        pltpu.VMEM((rows_e, 2 * hid), F32),
        pltpu.VMEM((rows_e, 2 * hid), F32),
        pltpu.VMEM((n_y, rows_m, W), BF16),
        pltpu.VMEM((n_y, rows_e, W), BF16),
        pltpu.VMEM((rows_m, width), BF16),
        pltpu.VMEM((rows_e, width), BF16),
        pltpu.VMEM((rows_m, L), F32),
        pltpu.VMEM((rows_e, L), F32),
        pltpu.VMEM((width, 3 * W), BF16),
        pltpu.VMEM((W, width), BF16),
        pltpu.VMEM((2 * hid, width), BF16),
        pltpu.VMEM((2 * hid, width), BF16),
        pltpu.VMEM((2 * hid, width), BF16),
        pltpu.VMEM((2, 3, L), F32),
        pltpu.VMEM((8, tokens), jnp.int32),
        pltpu.VMEM((8, tokens), F32),
        pltpu.VMEM((tokens, L), BF16),
        pltpu.VMEM((n_ep, stride, L), BF16),
        pltpu.VMEM((2, n_ep, stride, L), BF16),
        pltpu.VMEM((8 + rows_m, W), F32),
        pltpu.VMEM((rows_m, W), F32),
        pltpu.VMEM((rows_m, W), BF16),
        pltpu.VMEM((rows_e, 2 * hid), BF16),
        pltpu.VMEM((mix_slots, rows_m // MIX_PARTS, W), BF16),
        pltpu.VMEM((mix_slots, rows_m // MIX_PARTS, W), BF16),
        pltpu.VMEM((ex_slots, rows_e // Z, W), BF16),
        pltpu.VMEM((ex_slots, rows_e // Z, W), BF16),
        pltpu.VMEM((rows_m, L), BF16),
        pltpu.VMEM((2, n_ep, stride, L), BF16),
        pltpu.VMEM((n_ep, stride, L), BF16),
        pltpu.VMEM((2, rows_m, W), F32),
        pltpu.VMEM((2, rows_e, W), F32),
        dma((ex_slots,)),
        dma((ex_slots,)),
        dma((6,)),
        dma((Z,)),
        dma((5,)),
        dma((5,)),
        dma((5,)),
        dma((4,)),
        dma((7,)),
        pltpu.SemaphoreType.REGULAR((1,)),
        pltpu.VMEM((rows_m, 3 * W), F32),
    ]
    both = pl.pallas_call(
        functools.partial(kernel, n_ep, n_y, cap, stride),
        out_shape=pltpu.VMEM((mix_input.shape[0] + tok, L), BF16),
        in_specs=[any_spec] * 14,
        out_specs=vmem,
        scratch_shapes=scratch,
        compiler_params=pltpu.CompilerParams(
            collective_id=0, has_side_effects=True, vmem_limit_bytes=56 * 1024 * 1024
        ),
    )(
        mix_input,
        mix_gain.reshape(1, width),
        gate_b_weight,
        gate_c_weight,
        value_weight,
        conv_weight,
        out_weight,
        expert_input,
        expert_gain.reshape(1, width),
        routes.T,
        route_weight.T,
        jnp.swapaxes(expert_gate, 1, 2)[0],
        jnp.swapaxes(expert_up, 1, 2)[0],
        expert_down[0],
    )
    return both[: mix_input.shape[0]], both[mix_input.shape[0] :]


def solution(mesh):
    in_specs = (
        P("ep", "tp"),
        P(),
        P(None, "tp"),
        P(None, "tp"),
        P(None, "tp"),
        P(None, "tp"),
        P("tp", None),
        P("ep", "tp"),
        P(),
        P("ep", None),
        P("ep", None),
        P("ep", None, "tp"),
        P("ep", None, "tp"),
        P("ep", "tp", None),
    )
    out_specs = (P("ep", "tp"), P("ep", "tp"))
    return jax.shard_map(local, mesh=mesh, in_specs=in_specs, out_specs=out_specs, check_vma=False)
```

```python
import functools

import jax
import jax.numpy as jnp
from jax import lax
from jax.experimental import pallas as pl
from jax.experimental.pallas import tpu as pltpu
from jax.sharding import PartitionSpec as P

epsilon = 1e-06
routed_scale = 2.5
MESH = pl.DeviceIdType.MESH
F32 = jnp.float32
BF16 = jnp.bfloat16
L = 128
W = 2 * L
MIX_PARTS = 4
Z = 8
OFFS = (0, 1, -1, 2, -2, 3, -3, 4)


def mm(a, b):
    return jnp.dot(a, b, preferred_element_type=F32)


def mm_nt(a, b):
    return lax.dot_general(a, b, (((1,), (1,)), ((), ())), preferred_element_type=F32)


def kernel(*args):
    for core in range(2):

        @pl.when(lax.rem(lax.axis_index("tp"), 2) == core)
        def _():
            body(core, *args)


def body(
    c,
    n_ep,
    n_y,
    cap,
    stride,
    mix_in,
    mix_gain_in,
    gb,
    gc,
    vw,
    cw,
    ow,
    ex_in_in,
    ex_gain_in,
    routes_in,
    scores_in,
    eg,
    eu,
    ed,
    out,
    gain,
    routes,
    scores,
    ex_in,
    acc_gate,
    acc_up,
    xm,
    xe,
    xsm,
    xse,
    ssm,
    sse,
    wm,
    wo,
    wg,
    wu,
    wd,
    wc,
    rt,
    tpad,
    xpad,
    dsend,
    rbuf,
    prod,
    outer,
    gated,
    act,
    rs_m_send,
    rs_m_recv,
    rs_e_send,
    rs_e_recv,
    ymo,
    ysend,
    yrecv,
    rsend,
    ret,
    pre_m,
    pre_e,
    ag_sem,
    rs_sem,
    s_sem,
    d_sem,
    w_local,
    w_send,
    w_recv,
    i_sem,
    misc,
    go,
    acc_mix,
):
    ep = lax.axis_index("ep")
    tp = lax.axis_index("tp")
    y = tp // 2
    partner = 2 * y + 1 - c
    n_x = n_ep // Z
    z, x_own = ep // n_x, lax.rem(ep, n_x)
    long, short = n_y // 2, n_y - 1 - n_y // 2
    ring_tp = (2 * lax.rem(y + n_y - 1, n_y) + c, 2 * lax.rem(y + 1, n_y) + c)
    sign = (1, -1)
    hid = wg.shape[0] // 2
    tok, top = ex_in.shape[0], routes.shape[0]
    rows_m = xm.shape[1]
    x, xs, ss = ((xm, xsm, ssm), (xe, xse, sse))[c]
    send, recv, pre = ((rs_m_send, rs_m_recv, pre_m), (rs_e_send, rs_e_recv, pre_e))[c]
    parts = (MIX_PARTS, Z)[c]
    rows = x.shape[1] // parts

    def hops(way, part):
        return long if way == part % 2 else short

    order = [(way, part) for part in range(parts) for way in range(2)]
    last_first = [(way, part) for part in reversed(range(parts)) for way in range(2)]
    place = {}
    for step in range(long):
        for way, part in order:
            if step < hops(way, part):
                place[way, part, step] = len(place)

    def remote(src, dst, send_sem, recv_sem, device):
        return pltpu.make_async_remote_copy(
            src_ref=src,
            dst_ref=dst,
            send_sem=send_sem,
            recv_sem=recv_sem,
            device_id=device,
            device_id_type=MESH,
        )

    def sent(ref, sem):
        remote(ref, ref, sem, sem, (ep, partner)).wait_send()

    def received(ref, sem):
        remote(ref, ref, sem, sem, (ep, partner)).wait_recv()

    barrier = pltpu.get_barrier_semaphore()

    def along_x(off, act_on):
        def one(j, carry):
            act_on(lax.rem(z + off + Z, Z) * n_x + lax.rem(x_own + j, n_x))
            return carry

        lax.fori_loop(1 if off == 0 else 0, n_x, one, 0)

    small = [
        pltpu.make_async_copy(src, dst, i_sem.at[i])
        for i, (src, dst) in enumerate(
            (
                (routes_in, routes),
                (scores_in, scores),
                (ex_in_in, ex_in),
                ((mix_gain_in, ex_gain_in)[c], gain),
            )
        )
    ]
    for copy in small:
        copy.start()

    def greet(e):
        pl.semaphore_signal(barrier, inc=1, device_id=(e, 2 * y), device_id_type=MESH)
        pl.semaphore_signal(barrier, inc=1, device_id=(e, 2 * y + 1), device_id_type=MESH)

    for off in reversed(OFFS):
        along_x(off, greet)
    other_tp = tuple(t + 1 - 2 * c for t in ring_tp)
    for t in ring_tp + other_tp + (partner,):
        pl.semaphore_signal(barrier, inc=1, device_id=(ep, t), device_id_type=MESH)

    def weight_slots(core, who):
        if core == 0:
            return (
                (gb, wm.at[:, pl.ds(who * L, L)]),
                (gc, wm.at[:, pl.ds(W + who * L, L)]),
                (vw, wm.at[:, pl.ds(2 * W + who * L, L)]),
                (cw, wc.at[who]),
                (ow, wo.at[pl.ds(who * L, L)]),
            )
        return (
            (eg, wg.at[pl.ds(who * hid, hid)]),
            (eu, wu.at[pl.ds(who * hid, hid)]),
            (ed, wd.at[pl.ds(who * hid, hid)]),
        )

    own_weights = [
        pltpu.make_async_copy(src, dst, w_local.at[i])
        for i, (src, dst) in enumerate(weight_slots(c, c))
    ]
    give_weights = [
        remote(src, dst, w_send.at[i], w_recv.at[i], (ep, partner))
        for i, (src, dst) in enumerate(weight_slots(1 - c, c))
    ]
    if c == 0:
        own_mix = pltpu.make_async_copy(mix_in, xm.at[y, :, pl.ds(0, L)], misc.at[0])
        own_mix.start()
    else:
        own_mix = pltpu.make_async_copy(mix_in, ymo, misc.at[0])
        own_mix.start()
    for copy in own_weights:
        copy.start()

    def take_weights(lo, hi):
        for i in range(lo, hi):
            own_weights[i].wait()
            received(weight_slots(c, 1 - c)[i][1], w_recv.at[i])

    for copy in small:
        copy.wait()

    slots_all = n_ep * stride
    rt[...] = jnp.full(rt.shape, -1, jnp.int32)
    rt[0:top, 0:tok] = routes[...]
    tpad[...] = jnp.zeros_like(tpad)
    total_score = scores[0:1, :] + scores[1:2, :]
    tpad[2:3, 0:tok] = scores[0:1, :] / total_score * routed_scale
    tpad[3:4, 0:tok] = scores[1:2, :] / total_score * routed_scale
    xpad[...] = jnp.zeros_like(xpad)
    xpad[0:tok, :] = ex_in[...]
    tokens = rt.shape[1]
    experts = lax.broadcasted_iota(jnp.int32, (n_ep, tokens), 0)
    ones = [(experts == rt[k : k + 1, :]).astype(F32) for k in range(top)]
    before = (
        lax.broadcasted_iota(jnp.int32, (tokens, tokens), 0)
        < lax.broadcasted_iota(jnp.int32, (tokens, tokens), 1)
    ).astype(F32)
    ranks = mm((ones[0] + ones[1]).astype(BF16), before.astype(BF16))
    rows_iota = lax.broadcasted_iota(jnp.int32, (slots_all, tokens), 0)
    table = None
    for k in range(top):
        rank = jnp.sum(ranks * ones[k], axis=0, keepdims=True)
        slot = rt[k : k + 1, :] * stride + rank.astype(jnp.int32)
        tpad[k : k + 1, :] = slot.astype(F32)
        here = rows_iota == slot
        table = here if table is None else table | here
    outgoing = mm(table.astype(F32).astype(BF16), xpad[...]).astype(BF16)
    dsend[...] = outgoing.reshape(dsend.shape)
    ss[...] = jnp.zeros_like(ss)

    pl.semaphore_wait(barrier, 2 * (n_ep - 1) + 5)

    own_mix.wait()
    block = xm.at[y, :, pl.ds(0, L)] if c == 0 else ymo
    first_tp = ring_tp if c == 0 else other_tp
    mix_rows = rows_m // MIX_PARTS
    for part in range(MIX_PARTS):
        span = pl.ds(part * mix_rows, mix_rows)
        for way in range(2):
            if n_y > 2 or way == part % 2:
                remote(
                    block.at[span],
                    xm.at[y, span, pl.ds(c * L, L)],
                    misc.at[1 + way],
                    ag_sem.at[part * long],
                    (ep, first_tp[way]),
                ).start()
    if c == 1:
        give_mix = remote(ymo, xm.at[y, :, pl.ds(L, L)], s_sem.at[6], misc.at[7], (ep, partner))
        give_mix.start()

    def dispatch_copy(index, e):
        return remote(
            dsend.at[e],
            rbuf.at[c, index * n_x + x_own],
            s_sem.at[0],
            d_sem.at[index],
            (e, 2 * y + 1),
        )

    if c == 1:
        rbuf[1, x_own] = dsend[ep]
    else:
        dispatch_copy(0, ep).start()
    for index, off in enumerate(OFFS):
        along_x(-off, lambda e: dispatch_copy(index, e).start())
    for copy in give_weights:
        copy.start()

    def gather_block(way, part, step):
        origin = lax.rem(y + sign[way] * step + n_y, n_y)
        return x.at[origin, pl.ds(part * rows, rows)]

    def gather_send(way, part, step):
        block = gather_block(way, part, step)
        sem = ag_sem.at[part * long + step]
        remote(block, block, s_sem.at[1], sem, (ep, ring_tp[way])).start()

    def gather_start(part):
        for way in range(2):
            if hops(way, part) > 0:
                gather_send(way, part, 0)

    def gather_step(step, some):
        for part in some:
            ways = [way for way in range(2) if step < hops(way, part)]
            received(x.at[0, pl.ds(0, len(ways) * rows)], ag_sem.at[part * long + step])
            for way in ways:
                if step + 1 < hops(way, part):
                    gather_send(way, part, step + 1)

    def scale(origin):
        cols = pl.ds(pl.multiple_of(origin * W, W), W)
        wide = x[origin].astype(F32)
        square = wide * wide
        ss[...] += square[:, :L] + square[:, L:]
        xs[:, cols] = (wide * gain[:, cols]).astype(BF16)

    def origins_of(step):
        found = [lax.rem(y + step + 1, n_y)]
        if step < long - 1:
            found.append(lax.rem(y - step - 1 + n_y, n_y))
        return found

    def scale_step(step):
        for origin in origins_of(step):
            scale(origin)

    def factor_of(lo=0, hi=x.shape[1]):
        return lax.rsqrt(jnp.sum(ss[lo:hi], axis=1, keepdims=True) / (n_y * W) + epsilon)

    left, right = ((gated, wo), (act, wd))[c]

    def sum_slot(way, part, step):
        return place[way, part, step - (long - hops(way, part))]

    def sum_wait(part, step):
        count = sum(step >= long - hops(way, part) for way in range(2))
        received(recv.at[pl.ds(0, count)], rs_sem.at[part * long + step])

    def sum_in(way, part, step):
        return recv[sum_slot(way, part, step)].astype(F32)

    def prepare(step, lo=0, hi=x.shape[1]):
        for way in range(2 if 0 < step < long else 1):
            dest = y if step == long else lax.rem(y - sign[way] * (long - step) + n_y, n_y)
            cols = pl.ds(pl.multiple_of(dest * W, W), W)
            pre[way, lo:hi] = mm(left[lo:hi], right[:, cols])

    def sum_sends(step, some):
        for way, part in last_first:
            first = long - hops(way, part)
            if part not in some:
                continue
            if way == 0 and step > 0:
                sum_wait(part, step - 1)
            if step < first:
                continue
            value = pre[way if step > 0 else 0, part * rows : part * rows + rows]
            if step > first:
                value = value + sum_in(way, part, step - 1)
            slot = sum_slot(way, part, step)
            send[slot] = value.astype(BF16)
            remote(
                send.at[slot],
                recv.at[slot],
                s_sem.at[2],
                rs_sem.at[part * long + step],
                (ep, ring_tp[way]),
            ).start()

    def sum_step(step):
        sum_sends(step, range(parts))
        prepare(step + 1)

    def sum_result(part):
        value = pre[0, part * rows : part * rows + rows]
        sum_wait(part, long - 1)
        for way in range(2):
            if hops(way, part) > 0:
                value = value + sum_in(way, part, long - 1)
        return value.astype(BF16)

    def slot_table(shape, row_dim):
        row = lax.broadcasted_iota(jnp.int32, shape, row_dim)
        slot = lax.broadcasted_iota(jnp.int32, shape, 1 - row_dim)
        group = (row * (65536 // cap + 1)) >> 16
        return (slot - row == group * (stride - cap)).astype(F32).astype(BF16)

    if c == 0:
        received(ymo, misc.at[7])
        scale(y)
        for step in range(long):
            gather_step(step, range(parts))
            scale_step(step)
            origins = origins_of(step)
            if step == 0:
                origins.append(y)
                take_weights(0, 4)
            value = None if step == 0 else acc_mix[...]
            for origin in origins:
                cols = pl.ds(pl.multiple_of(origin * W, W), W)
                term = mm(xs[:, cols], wm[cols, :])
                value = term if value is None else value + term
            acc_mix[...] = value

        factor = factor_of()

        def product(lo, hi):
            part = factor[lo:hi]
            inner = acc_mix[lo:hi, W : 2 * W] * part
            prod[8 + lo : 8 + hi, :] = inner * (acc_mix[lo:hi, 2 * W :] * part)

        product(rows_m - 16, rows_m)
        halo = remote(
            prod.at[pl.ds(rows_m, 8)],
            prod.at[pl.ds(0, 8)],
            misc.at[3],
            misc.at[4],
            (lax.rem(ep + 1, n_ep), tp),
        )

        @pl.when(ep < n_ep - 1)
        def _():
            halo.start()

        product(0, rows_m - 16)
        outer[...] = acc_mix[:, :W] * factor

        take_weights(4, 5)

        def convolve(lo, hi):
            for h in range(2):
                cols = slice(h * L, h * L + L)
                convolved = (
                    wc[h, 0:1] * prod[6 + lo : 6 + hi, cols]
                    + wc[h, 1:2] * prod[7 + lo : 7 + hi, cols]
                    + wc[h, 2:3] * prod[8 + lo : 8 + hi, cols]
                )
                gated[lo:hi, cols] = (outer[lo:hi, cols] * convolved).astype(BF16)

        convolve(16, rows_m)
        prepare(0, rows, rows_m)
        sum_sends(0, range(1, parts))

        @pl.when(ep > 0)
        def _():
            halo.wait_recv()

        @pl.when(ep == 0)
        def _():
            prod[0:8, :] = jnp.zeros((8, W), F32)

        convolve(0, 16)
        prepare(0, 0, rows)
        sum_sends(0, (0,))
        prepare(1)
        for step in range(1, long):
            if step == long - 1:
                pl.semaphore_wait(go.at[0], 1)
            sum_step(step)
        if long == 1:
            pl.semaphore_wait(go.at[0], 1)
        give_out = remote(ysend, yrecv, misc.at[5], misc.at[6], (ep, partner))
        for part in range(parts):
            value = sum_result(part)
            out[part * rows : part * rows + rows, :] = value[:, :L]
            ysend[part * rows : part * rows + rows, :] = value[:, L:]
        give_out.start()
    else:

        def take_dispatch(part):
            count = 2 * n_x - (1 if part == 0 else 0)
            received(dsend.at[pl.ds(0, count)], d_sem.at[part])
            pick = slot_table((rows, n_x * stride), 0)
            for cs in range(2):
                block = rbuf[cs, pl.ds(part * n_x, n_x)].reshape(n_x * stride, L)
                piece = mm(pick, block).astype(BF16)
                xe[y, part * rows : part * rows + rows, cs * L : cs * L + L] = piece
            gather_start(part)

        def project(step):
            origins = origins_of(step)
            if step == 0:
                origins.append(y)
                take_weights(0, 2)
            for acc, weight in ((acc_gate, wg), (acc_up, wu)):
                value = None if step == 0 else acc[...]
                for origin in origins:
                    cols = pl.ds(pl.multiple_of(origin * W, W), W)
                    term = mm_nt(xs[:, cols], weight[:, cols])
                    value = term if value is None else value + term
                acc[...] = value

        for part in range(parts):
            take_dispatch(part)
            if part >= parts // 2 + 1:
                gather_step(0, (part - parts // 2 - 1,))
        scale(y)
        gather_step(0, range(parts // 2 - 1, parts))
        if long > 1:
            gather_step(1, range(parts))
        scale_step(0)
        project(0)
        for step in range(1, long):
            if step > 1:
                gather_step(step, range(parts))
            scale_step(step)
            project(step)
        take_weights(2, 3)
        half = x.shape[1] // 2
        for lo in (half, 0):
            factor = factor_of(lo, lo + half)
            gate = acc_gate[lo : lo + half] * factor
            up = acc_up[lo : lo + half] * factor
            act[lo : lo + half] = (gate / (1.0 + jnp.exp(-gate)) * up).astype(BF16)
            prepare(0, lo, lo + half)
            sum_sends(0, range(lo // rows, (lo + half) // rows))
        prepare(1)
        for step in range(1, long):
            sum_step(step)

        def return_copy(part, j, cs):
            return remote(
                rsend.at[cs, part * n_x + j],
                ret.at[ep],
                s_sem.at[3 + cs],
                s_sem.at[5],
                (lax.rem(z + OFFS[part] + Z, Z) * n_x + j, 2 * y + cs),
            )

        spread_table = slot_table((n_x * stride, rows), 1)
        for part in reversed(range(parts)):
            spread = mm(spread_table, sum_result(part)).astype(BF16)
            if part == 7:
                pl.semaphore_signal(
                    go.at[0], inc=1, device_id=(ep, partner), device_id_type=MESH
                )
            for cs in range(2):
                piece = spread[:, cs * L : cs * L + L].reshape(n_x, stride, L)
                rsend[cs, part * n_x : part * n_x + n_x] = piece

            def one(i, carry):
                j = lax.rem(x_own + i, n_x)
                return_copy(part, j, 0).start()
                if part > 0:
                    return_copy(part, j, 1).start()
                else:

                    @pl.when(j != x_own)
                    def _():
                        return_copy(part, j, 1).start()

                return carry

            lax.fori_loop(0, n_x, one, 0)
        ret[ep] = rsend[1, x_own]

    tcol = jnp.transpose(tpad[...])
    lane = lax.broadcasted_iota(jnp.int32, (tok, slots_all), 1)
    picks = [
        (lane == tcol[0:tok, k : k + 1].astype(jnp.int32)).astype(F32).astype(BF16)
        for k in range(top)
    ]
    for i in range(len(give_weights)):
        give_weights[i].wait_send()
    sent(dsend.at[pl.ds(0, n_ep - c)], s_sem.at[0])
    sent(ymo, misc.at[1])
    sent(ymo, misc.at[2])
    sent(x.at[pl.ds(0, n_y - (1, 3)[1 - c])], s_sem.at[1])
    sent(send, s_sem.at[2])
    if c == 0:

        @pl.when(ep < n_ep - 1)
        def _():
            halo.wait_send()

        give_out.wait_send()
    else:
        give_mix.wait_send()
        received(yrecv, misc.at[6])
        out[pl.ds(0, rows_m), :] = yrecv[...]
        sent(rsend.at[0], s_sem.at[3])
        sent(rsend.at[1, pl.ds(0, n_ep - 1)], s_sem.at[4])
    received(dsend.at[pl.ds(0, n_ep - c)], s_sem.at[5])
    back = ret[...].reshape(slots_all, L)
    total = None
    for k in range(top):
        term = mm(picks[k], back) * tcol[0:tok, 2 + k : 3 + k]
        total = term if total is None else total + term
    out[pl.ds(rows_m, tok), :] = total.astype(BF16)


def local(
    mix_input,
    mix_gain,
    gate_b_weight,
    gate_c_weight,
    value_weight,
    conv_weight,
    out_weight,
    expert_input,
    expert_gain,
    routes,
    route_weight,
    expert_gate,
    expert_up,
    expert_down,
):
    n_ep, n_tp = lax.axis_size("ep"), lax.axis_size("tp")
    n_y = n_tp // 2
    tok, top = routes.shape
    cap = 2 * tok * top // n_ep
    stride = -(-cap // 8) * 8
    rows_m = mix_input.shape[0]
    rows_e = n_ep * cap
    width = mix_gain.shape[0]
    hid = expert_gate.shape[2]
    tokens = -(-tok // L) * L
    mix_slots, ex_slots = MIX_PARTS * (n_y - 1), Z * (n_y - 1)
    dma = pltpu.SemaphoreType.DMA
    any_spec = pl.BlockSpec(memory_space=pl.ANY)
    vmem = pl.BlockSpec(memory_space=pltpu.VMEM)
    scratch = [
        pltpu.VMEM((1, width), F32),
        pltpu.VMEM((top, tok), jnp.int32),
        pltpu.VMEM((top, tok), F32),
        pltpu.VMEM((tok, L), BF16),
        pltpu.VMEM((rows_e, 2 * hid), F32),
        pltpu.VMEM((rows_e, 2 * hid), F32),
        pltpu.VMEM((n_y, rows_m, W), BF16),
        pltpu.VMEM((n_y, rows_e, W), BF16),
        pltpu.VMEM((rows_m, width), BF16),
        pltpu.VMEM((rows_e, width), BF16),
        pltpu.VMEM((rows_m, L), F32),
        pltpu.VMEM((rows_e, L), F32),
        pltpu.VMEM((width, 3 * W), BF16),
        pltpu.VMEM((W, width), BF16),
        pltpu.VMEM((2 * hid, width), BF16),
        pltpu.VMEM((2 * hid, width), BF16),
        pltpu.VMEM((2 * hid, width), BF16),
        pltpu.VMEM((2, 3, L), F32),
        pltpu.VMEM((8, tokens), jnp.int32),
        pltpu.VMEM((8, tokens), F32),
        pltpu.VMEM((tokens, L), BF16),
        pltpu.VMEM((n_ep, stride, L), BF16),
        pltpu.VMEM((2, n_ep, stride, L), BF16),
        pltpu.VMEM((8 + rows_m, W), F32),
        pltpu.VMEM((rows_m, W), F32),
        pltpu.VMEM((rows_m, W), BF16),
        pltpu.VMEM((rows_e, 2 * hid), BF16),
        pltpu.VMEM((mix_slots, rows_m // MIX_PARTS, W), BF16),
        pltpu.VMEM((mix_slots, rows_m // MIX_PARTS, W), BF16),
        pltpu.VMEM((ex_slots, rows_e // Z, W), BF16),
        pltpu.VMEM((ex_slots, rows_e // Z, W), BF16),
        pltpu.VMEM((rows_m, L), BF16),
        pltpu.VMEM((rows_m, L), BF16),
        pltpu.VMEM((rows_m, L), BF16),
        pltpu.VMEM((2, n_ep, stride, L), BF16),
        pltpu.VMEM((n_ep, stride, L), BF16),
        pltpu.VMEM((2, rows_m, W), F32),
        pltpu.VMEM((2, rows_e, W), F32),
        dma((Z * (n_y // 2),)),
        dma((Z * (n_y // 2),)),
        dma((7,)),
        dma((Z,)),
        dma((5,)),
        dma((5,)),
        dma((5,)),
        dma((4,)),
        dma((8,)),
        pltpu.SemaphoreType.REGULAR((1,)),
        pltpu.VMEM((rows_m, 3 * W), F32),
    ]
    both = pl.pallas_call(
        functools.partial(kernel, n_ep, n_y, cap, stride),
        out_shape=pltpu.VMEM((mix_input.shape[0] + tok, L), BF16),
        in_specs=[any_spec] * 14,
        out_specs=vmem,
        scratch_shapes=scratch,
        compiler_params=pltpu.CompilerParams(
            collective_id=0, has_side_effects=True, vmem_limit_bytes=56 * 1024 * 1024
        ),
    )(
        mix_input,
        mix_gain.reshape(1, width),
        gate_b_weight,
        gate_c_weight,
        value_weight,
        conv_weight,
        out_weight,
        expert_input,
        expert_gain.reshape(1, width),
        routes.T,
        route_weight.T,
        jnp.swapaxes(expert_gate, 1, 2)[0],
        jnp.swapaxes(expert_up, 1, 2)[0],
        expert_down[0],
    )
    return both[: mix_input.shape[0]], both[mix_input.shape[0] :]


def solution(mesh):
    in_specs = (
        P("ep", "tp"),
        P(),
        P(None, "tp"),
        P(None, "tp"),
        P(None, "tp"),
        P(None, "tp"),
        P("tp", None),
        P("ep", "tp"),
        P(),
        P("ep", None),
        P("ep", None),
        P("ep", None, "tp"),
        P("ep", None, "tp"),
        P("ep", "tp", None),
    )
    out_specs = (P("ep", "tp"), P("ep", "tp"))
    return jax.shard_map(local, mesh=mesh, in_specs=in_specs, out_specs=out_specs, check_vma=False)
```

```python
import functools

import jax
import jax.numpy as jnp
from jax import lax
from jax.experimental import pallas as pl
from jax.experimental.pallas import tpu as pltpu
from jax.sharding import PartitionSpec as P

epsilon = 1e-06
routed_scale = 2.5
MESH = pl.DeviceIdType.MESH
F32 = jnp.float32
BF16 = jnp.bfloat16
L = 128
W = 2 * L
MIX_PARTS = 4
Z = 8
OFFS = (0, 1, -1, 2, -2, 3, -3, 4)


def mm(a, b):
    return jnp.dot(a, b, preferred_element_type=F32)


def mm_nt(a, b):
    return lax.dot_general(a, b, (((1,), (1,)), ((), ())), preferred_element_type=F32)


def kernel(*args):
    for core in range(2):

        @pl.when(lax.rem(lax.axis_index("tp"), 2) == core)
        def _():
            body(core, *args)


def body(
    c,
    n_ep,
    n_y,
    cap,
    stride,
    mix_in,
    mix_gain_in,
    gb,
    gc,
    vw,
    cw,
    ow,
    ex_in_in,
    ex_gain_in,
    routes_in,
    scores_in,
    eg,
    eu,
    ed,
    out,
    gain,
    routes,
    scores,
    ex_in,
    acc_gate,
    acc_up,
    xm,
    xe,
    xsm,
    xse,
    ssm,
    sse,
    wm,
    wo,
    wg,
    wu,
    wd,
    wc,
    rt,
    tpad,
    xpad,
    dsend,
    rbuf,
    prod,
    outer,
    gated,
    act,
    rs_m_send,
    rs_m_recv,
    rs_e_send,
    rs_e_recv,
    ymo,
    ysend,
    yrecv,
    rsend,
    ret,
    pre_m,
    pre_e,
    ag_sem,
    rs_sem,
    s_sem,
    d_sem,
    w_local,
    w_send,
    w_recv,
    i_sem,
    misc,
    go,
    acc_mix,
):
    ep = lax.axis_index("ep")
    tp = lax.axis_index("tp")
    y = tp // 2
    partner = 2 * y + 1 - c
    n_x = n_ep // Z
    z, x_own = ep // n_x, lax.rem(ep, n_x)
    long, short = n_y // 2, n_y - 1 - n_y // 2
    ring_tp = (2 * lax.rem(y + n_y - 1, n_y) + c, 2 * lax.rem(y + 1, n_y) + c)
    sign = (1, -1)
    hid = wg.shape[0] // 2
    tok, top = ex_in.shape[0], routes.shape[0]
    rows_m = xm.shape[1]
    x, xs, ss = ((xm, xsm, ssm), (xe, xse, sse))[c]
    send, recv, pre = ((rs_m_send, rs_m_recv, pre_m), (rs_e_send, rs_e_recv, pre_e))[c]
    parts = (MIX_PARTS, Z)[c]
    rows = x.shape[1] // parts

    def hops(way, part):
        return long if way == part % 2 else short

    order = [(way, part) for part in range(parts) for way in range(2)]
    last_first = [(way, part) for part in reversed(range(parts)) for way in range(2)]
    place = {}
    for step in range(long):
        for way, part in order:
            if step < hops(way, part):
                place[way, part, step] = len(place)

    def remote(src, dst, send_sem, recv_sem, device):
        return pltpu.make_async_remote_copy(
            src_ref=src,
            dst_ref=dst,
            send_sem=send_sem,
            recv_sem=recv_sem,
            device_id=device,
            device_id_type=MESH,
        )

    def sent(ref, sem):
        remote(ref, ref, sem, sem, (ep, partner)).wait_send()

    def received(ref, sem):
        remote(ref, ref, sem, sem, (ep, partner)).wait_recv()

    barrier = pltpu.get_barrier_semaphore()

    def along_x(off, act_on):
        def one(j, carry):
            act_on(lax.rem(z + off + Z, Z) * n_x + lax.rem(x_own + j, n_x))
            return carry

        lax.fori_loop(1 if off == 0 else 0, n_x, one, 0)

    small = [
        pltpu.make_async_copy(src, dst, i_sem.at[i])
        for i, (src, dst) in enumerate(
            (
                (routes_in, routes),
                (scores_in, scores),
                (ex_in_in, ex_in),
                ((mix_gain_in, ex_gain_in)[c], gain),
            )
        )
    ]
    for copy in small:
        copy.start()

    def greet(e):
        pl.semaphore_signal(barrier, inc=1, device_id=(e, 2 * y), device_id_type=MESH)
        pl.semaphore_signal(barrier, inc=1, device_id=(e, 2 * y + 1), device_id_type=MESH)

    for off in reversed(OFFS):
        along_x(off, greet)
    other_tp = tuple(t + 1 - 2 * c for t in ring_tp)
    for t in ring_tp + other_tp + (partner,):
        pl.semaphore_signal(barrier, inc=1, device_id=(ep, t), device_id_type=MESH)

    def weight_slots(core, who):
        if core == 0:
            return (
                (gb, wm.at[:, pl.ds(who * L, L)]),
                (gc, wm.at[:, pl.ds(W + who * L, L)]),
                (vw, wm.at[:, pl.ds(2 * W + who * L, L)]),
                (cw, wc.at[who]),
                (ow, wo.at[pl.ds(who * L, L)]),
            )
        return (
            (eg, wg.at[pl.ds(who * hid, hid)]),
            (eu, wu.at[pl.ds(who * hid, hid)]),
            (ed, wd.at[pl.ds(who * hid, hid)]),
        )

    own_weights = [
        pltpu.make_async_copy(src, dst, w_local.at[i])
        for i, (src, dst) in enumerate(weight_slots(c, c))
    ]
    give_weights = [
        remote(src, dst, w_send.at[i], w_recv.at[i], (ep, partner))
        for i, (src, dst) in enumerate(weight_slots(1 - c, c))
    ]
    if c == 0:
        own_mix = pltpu.make_async_copy(mix_in, xm.at[y, :, pl.ds(0, L)], misc.at[0])
        own_mix.start()
    else:
        own_mix = pltpu.make_async_copy(mix_in, ymo, misc.at[0])
        own_mix.start()
    for copy in own_weights:
        copy.start()

    def take_weights(lo, hi):
        for i in range(lo, hi):
            own_weights[i].wait()
            received(weight_slots(c, 1 - c)[i][1], w_recv.at[i])

    for copy in small:
        copy.wait()

    slots_all = n_ep * stride
    rt[...] = jnp.full(rt.shape, -1, jnp.int32)
    rt[0:top, 0:tok] = routes[...]
    tpad[...] = jnp.zeros_like(tpad)
    total_score = scores[0:1, :] + scores[1:2, :]
    tpad[2:3, 0:tok] = scores[0:1, :] / total_score * routed_scale
    tpad[3:4, 0:tok] = scores[1:2, :] / total_score * routed_scale
    xpad[...] = jnp.zeros_like(xpad)
    xpad[0:tok, :] = ex_in[...]
    tokens = rt.shape[1]
    experts = lax.broadcasted_iota(jnp.int32, (n_ep, tokens), 0)
    ones = [(experts == rt[k : k + 1, :]).astype(F32) for k in range(top)]
    before = (
        lax.broadcasted_iota(jnp.int32, (tokens, tokens), 0)
        < lax.broadcasted_iota(jnp.int32, (tokens, tokens), 1)
    ).astype(F32)
    ranks = mm((ones[0] + ones[1]).astype(BF16), before.astype(BF16))
    rows_iota = lax.broadcasted_iota(jnp.int32, (slots_all, tokens), 0)
    table = None
    for k in range(top):
        rank = jnp.sum(ranks * ones[k], axis=0, keepdims=True)
        slot = rt[k : k + 1, :] * stride + rank.astype(jnp.int32)
        tpad[k : k + 1, :] = slot.astype(F32)
        here = rows_iota == slot
        table = here if table is None else table | here
    outgoing = mm(table.astype(F32).astype(BF16), xpad[...]).astype(BF16)
    dsend[...] = outgoing.reshape(dsend.shape)
    ss[...] = jnp.zeros_like(ss)

    pl.semaphore_wait(barrier, 2 * (n_ep - 1) + 5)

    own_mix.wait()
    block = xm.at[y, :, pl.ds(0, L)] if c == 0 else ymo
    first_tp = ring_tp if c == 0 else other_tp
    mix_rows = rows_m // MIX_PARTS
    for part in range(MIX_PARTS):
        span = pl.ds(part * mix_rows, mix_rows)
        for way in range(2):
            if n_y > 2 or way == part % 2:
                remote(
                    block.at[span],
                    xm.at[y, span, pl.ds(c * L, L)],
                    misc.at[1 + way],
                    ag_sem.at[part * long],
                    (ep, first_tp[way]),
                ).start()
    if c == 1:
        give_mix = remote(ymo, xm.at[y, :, pl.ds(L, L)], s_sem.at[6], misc.at[7], (ep, partner))
        give_mix.start()

    def dispatch_copy(index, e):
        return remote(
            dsend.at[e],
            rbuf.at[c, index * n_x + x_own],
            s_sem.at[0],
            d_sem.at[index],
            (e, 2 * y + 1),
        )

    if c == 1:
        rbuf[1, x_own] = dsend[ep]
    else:
        dispatch_copy(0, ep).start()
    for index, off in enumerate(OFFS):
        along_x(-off, lambda e: dispatch_copy(index, e).start())
    for copy in give_weights:
        copy.start()

    def gather_block(way, part, step):
        origin = lax.rem(y + sign[way] * step + n_y, n_y)
        return x.at[origin, pl.ds(part * rows, rows)]

    def gather_send(way, part, step):
        block = gather_block(way, part, step)
        sem = ag_sem.at[part * long + step]
        remote(block, block, s_sem.at[1], sem, (ep, ring_tp[way])).start()

    def gather_start(part):
        for way in range(2):
            if hops(way, part) > 0:
                gather_send(way, part, 0)

    def gather_step(step, some):
        for part in some:
            ways = [way for way in range(2) if step < hops(way, part)]
            received(x.at[0, pl.ds(0, len(ways) * rows)], ag_sem.at[part * long + step])
            for way in ways:
                if step + 1 < hops(way, part):
                    gather_send(way, part, step + 1)

    def scale(origin):
        cols = pl.ds(pl.multiple_of(origin * W, W), W)
        wide = x[origin].astype(F32)
        square = wide * wide
        ss[...] += square[:, :L] + square[:, L:]
        xs[:, cols] = (wide * gain[:, cols]).astype(BF16)

    def origins_of(step):
        found = [lax.rem(y + step + 1, n_y)]
        if step < long - 1:
            found.append(lax.rem(y - step - 1 + n_y, n_y))
        return found

    def scale_step(step):
        for origin in origins_of(step):
            scale(origin)

    def factor_of(lo=0, hi=x.shape[1]):
        return lax.rsqrt(jnp.sum(ss[lo:hi], axis=1, keepdims=True) / (n_y * W) + epsilon)

    left, right = ((gated, wo), (act, wd))[c]

    def sum_slot(way, part, step):
        return place[way, part, step - (long - hops(way, part))]

    def sum_wait(part, step):
        count = sum(step >= long - hops(way, part) for way in range(2))
        received(recv.at[pl.ds(0, count)], rs_sem.at[part * long + step])

    def sum_in(way, part, step):
        return recv[sum_slot(way, part, step)].astype(F32)

    def prepare(step, lo=0, hi=x.shape[1]):
        for way in range(2 if 0 < step < long else 1):
            dest = y if step == long else lax.rem(y - sign[way] * (long - step) + n_y, n_y)
            cols = pl.ds(pl.multiple_of(dest * W, W), W)
            pre[way, lo:hi] = mm(left[lo:hi], right[:, cols])

    def sum_sends(step, some):
        for way, part in last_first:
            first = long - hops(way, part)
            if part not in some:
                continue
            if way == 0 and step > 0:
                sum_wait(part, step - 1)
            if step < first:
                continue
            value = pre[way if step > 0 else 0, part * rows : part * rows + rows]
            if step > first:
                value = value + sum_in(way, part, step - 1)
            slot = sum_slot(way, part, step)
            send[slot] = value.astype(BF16)
            remote(
                send.at[slot],
                recv.at[slot],
                s_sem.at[2],
                rs_sem.at[part * long + step],
                (ep, ring_tp[way]),
            ).start()

    def sum_step(step):
        sum_sends(step, range(parts))
        prepare(step + 1)

    def sum_result(part):
        value = pre[0, part * rows : part * rows + rows]
        sum_wait(part, long - 1)
        for way in range(2):
            if hops(way, part) > 0:
                value = value + sum_in(way, part, long - 1)
        return value.astype(BF16)

    def slot_table(shape, row_dim):
        row = lax.broadcasted_iota(jnp.int32, shape, row_dim)
        slot = lax.broadcasted_iota(jnp.int32, shape, 1 - row_dim)
        group = (row * (65536 // cap + 1)) >> 16
        return (slot - row == group * (stride - cap)).astype(F32).astype(BF16)

    if c == 0:
        received(ymo, misc.at[7])
        scale(y)
        for step in range(long):
            gather_step(step, range(parts))
            scale_step(step)
            origins = origins_of(step)
            if step == 0:
                origins.append(y)
                take_weights(0, 4)
            value = None if step == 0 else acc_mix[...]
            for origin in origins:
                cols = pl.ds(pl.multiple_of(origin * W, W), W)
                term = mm(xs[:, cols], wm[cols, :])
                value = term if value is None else value + term
            acc_mix[...] = value

        factor = factor_of()

        def product(lo, hi):
            part = factor[lo:hi]
            inner = acc_mix[lo:hi, W : 2 * W] * part
            prod[8 + lo : 8 + hi, :] = inner * (acc_mix[lo:hi, 2 * W :] * part)

        product(rows_m - 16, rows_m)
        halo = remote(
            prod.at[pl.ds(rows_m, 8)],
            prod.at[pl.ds(0, 8)],
            misc.at[3],
            misc.at[4],
            (lax.rem(ep + 1, n_ep), tp),
        )

        @pl.when(ep < n_ep - 1)
        def _():
            halo.start()

        product(0, rows_m - 16)
        outer[...] = acc_mix[:, :W] * factor

        take_weights(4, 5)

        def convolve(lo, hi):
            for h in range(2):
                cols = slice(h * L, h * L + L)
                convolved = (
                    wc[h, 0:1] * prod[6 + lo : 6 + hi, cols]
                    + wc[h, 1:2] * prod[7 + lo : 7 + hi, cols]
                    + wc[h, 2:3] * prod[8 + lo : 8 + hi, cols]
                )
                gated[lo:hi, cols] = (outer[lo:hi, cols] * convolved).astype(BF16)

        convolve(16, rows_m)
        prepare(0, rows, rows_m)
        sum_sends(0, range(1, parts))

        @pl.when(ep > 0)
        def _():
            halo.wait_recv()

        @pl.when(ep == 0)
        def _():
            prod[0:8, :] = jnp.zeros((8, W), F32)

        convolve(0, 16)
        prepare(0, 0, rows)
        sum_sends(0, (0,))
        prepare(1)
        for step in range(1, long):
            if step == long - 1:
                pl.semaphore_wait(go.at[0], 1)
            sum_step(step)
        if long == 1:
            pl.semaphore_wait(go.at[0], 1)
        give_out = remote(ysend, yrecv, misc.at[5], misc.at[6], (ep, partner))
        for part in range(parts):
            value = sum_result(part)
            out[part * rows : part * rows + rows, :] = value[:, :L]
            ysend[part * rows : part * rows + rows, :] = value[:, L:]
        give_out.start()
    else:

        def take_dispatch(part):
            count = 2 * n_x - (1 if part == 0 else 0)
            received(dsend.at[pl.ds(0, count)], d_sem.at[part])
            pick = slot_table((rows, n_x * stride), 0)
            for cs in range(2):
                block = rbuf[cs, pl.ds(part * n_x, n_x)].reshape(n_x * stride, L)
                piece = mm(pick, block).astype(BF16)
                xe[y, part * rows : part * rows + rows, cs * L : cs * L + L] = piece
            gather_start(part)

        def project(step):
            origins = origins_of(step)
            if step == 0:
                origins.append(y)
                take_weights(0, 2)
            for acc, weight in ((acc_gate, wg), (acc_up, wu)):
                value = None if step == 0 else acc[...]
                for origin in origins:
                    cols = pl.ds(pl.multiple_of(origin * W, W), W)
                    term = mm_nt(xs[:, cols], weight[:, cols])
                    value = term if value is None else value + term
                acc[...] = value

        for part in range(parts):
            take_dispatch(part)
            if part >= parts // 2 + 1:
                gather_step(0, (part - parts // 2 - 1,))
        scale(y)
        gather_step(0, range(parts // 2 - 1, parts))
        if long > 1:
            gather_step(1, range(parts))
        scale_step(0)
        project(0)
        for step in range(1, long):
            if step > 1:
                gather_step(step, range(parts))
            scale_step(step)
            project(step)
        take_weights(2, 3)
        half = x.shape[1] // 2
        for lo in (half, 0):
            factor = factor_of(lo, lo + half)
            gate = acc_gate[lo : lo + half] * factor
            up = acc_up[lo : lo + half] * factor
            act[lo : lo + half] = (gate / (1.0 + jnp.exp(-gate)) * up).astype(BF16)
            prepare(0, lo, lo + half)
            sum_sends(0, range(lo // rows, (lo + half) // rows))
        prepare(1)
        for step in range(1, long):
            sum_step(step)

        def return_copy(part, j, cs):
            return remote(
                rsend.at[cs, part * n_x + j],
                ret.at[ep],
                s_sem.at[3 + cs],
                s_sem.at[5],
                (lax.rem(z + OFFS[part] + Z, Z) * n_x + j, 2 * y + cs),
            )

        spread_table = slot_table((n_x * stride, rows), 1)
        for part in reversed(range(parts)):
            spread = mm(spread_table, sum_result(part)).astype(BF16)
            if part == 7:
                pl.semaphore_signal(
                    go.at[0], inc=1, device_id=(ep, partner), device_id_type=MESH
                )
            for cs in range(2):
                piece = spread[:, cs * L : cs * L + L].reshape(n_x, stride, L)
                rsend[cs, part * n_x : part * n_x + n_x] = piece

            def one(i, carry):
                j = lax.rem(x_own + i, n_x)
                return_copy(part, j, 0).start()
                if part > 0:
                    return_copy(part, j, 1).start()
                else:

                    @pl.when(j != x_own)
                    def _():
                        return_copy(part, j, 1).start()

                return carry

            lax.fori_loop(0, n_x, one, 0)
        ret[ep] = rsend[1, x_own]

    tcol = jnp.transpose(tpad[...])
    lane = lax.broadcasted_iota(jnp.int32, (tok, slots_all), 1)
    picks = [
        (lane == tcol[0:tok, k : k + 1].astype(jnp.int32)).astype(F32).astype(BF16)
        for k in range(top)
    ]
    for i in range(len(give_weights)):
        give_weights[i].wait_send()
    sent(dsend.at[pl.ds(0, n_ep - c)], s_sem.at[0])
    sent(ymo, misc.at[1])
    sent(ymo, misc.at[2])
    sent(x.at[pl.ds(0, n_y - (1, 3)[1 - c])], s_sem.at[1])
    sent(send, s_sem.at[2])
    if c == 0:

        @pl.when(ep < n_ep - 1)
        def _():
            halo.wait_send()

        give_out.wait_send()
    else:
        give_mix.wait_send()
        received(yrecv, misc.at[6])
        out[pl.ds(0, rows_m), :] = yrecv[...]
        sent(rsend.at[0], s_sem.at[3])
        sent(rsend.at[1, pl.ds(0, n_ep - 1)], s_sem.at[4])
    received(dsend.at[pl.ds(0, n_ep - c)], s_sem.at[5])
    back = ret[...].reshape(slots_all, L)
    total = None
    for k in range(top):
        term = mm(picks[k], back) * tcol[0:tok, 2 + k : 3 + k]
        total = term if total is None else total + term
    out[pl.ds(rows_m, tok), :] = total.astype(BF16)


def deliver(both, mix_out, ex_out, sems):
    rows = mix_out.shape[0]
    copies = (
        pltpu.make_async_copy(both.at[pl.ds(0, rows)], mix_out, sems.at[0]),
        pltpu.make_async_copy(both.at[pl.ds(rows, ex_out.shape[0])], ex_out, sems.at[1]),
    )
    for copy in copies:
        copy.start()
    for copy in copies:
        copy.wait()


def local(
    mix_input,
    mix_gain,
    gate_b_weight,
    gate_c_weight,
    value_weight,
    conv_weight,
    out_weight,
    expert_input,
    expert_gain,
    routes,
    route_weight,
    expert_gate,
    expert_up,
    expert_down,
):
    n_ep, n_tp = lax.axis_size("ep"), lax.axis_size("tp")
    n_y = n_tp // 2
    tok, top = routes.shape
    cap = 2 * tok * top // n_ep
    stride = -(-cap // 8) * 8
    rows_m = mix_input.shape[0]
    rows_e = n_ep * cap
    width = mix_gain.shape[0]
    hid = expert_gate.shape[2]
    tokens = -(-tok // L) * L
    mix_slots, ex_slots = MIX_PARTS * (n_y - 1), Z * (n_y - 1)
    dma = pltpu.SemaphoreType.DMA
    any_spec = pl.BlockSpec(memory_space=pl.ANY)
    vmem = pl.BlockSpec(memory_space=pltpu.VMEM)
    scratch = [
        pltpu.VMEM((1, width), F32),
        pltpu.VMEM((top, tok), jnp.int32),
        pltpu.VMEM((top, tok), F32),
        pltpu.VMEM((tok, L), BF16),
        pltpu.VMEM((rows_e, 2 * hid), F32),
        pltpu.VMEM((rows_e, 2 * hid), F32),
        pltpu.VMEM((n_y, rows_m, W), BF16),
        pltpu.VMEM((n_y, rows_e, W), BF16),
        pltpu.VMEM((rows_m, width), BF16),
        pltpu.VMEM((rows_e, width), BF16),
        pltpu.VMEM((rows_m, L), F32),
        pltpu.VMEM((rows_e, L), F32),
        pltpu.VMEM((width, 3 * W), BF16),
        pltpu.VMEM((W, width), BF16),
        pltpu.VMEM((2 * hid, width), BF16),
        pltpu.VMEM((2 * hid, width), BF16),
        pltpu.VMEM((2 * hid, width), BF16),
        pltpu.VMEM((2, 3, L), F32),
        pltpu.VMEM((8, tokens), jnp.int32),
        pltpu.VMEM((8, tokens), F32),
        pltpu.VMEM((tokens, L), BF16),
        pltpu.VMEM((n_ep, stride, L), BF16),
        pltpu.VMEM((2, n_ep, stride, L), BF16),
        pltpu.VMEM((8 + rows_m, W), F32),
        pltpu.VMEM((rows_m, W), F32),
        pltpu.VMEM((rows_m, W), BF16),
        pltpu.VMEM((rows_e, 2 * hid), BF16),
        pltpu.VMEM((mix_slots, rows_m // MIX_PARTS, W), BF16),
        pltpu.VMEM((mix_slots, rows_m // MIX_PARTS, W), BF16),
        pltpu.VMEM((ex_slots, rows_e // Z, W), BF16),
        pltpu.VMEM((ex_slots, rows_e // Z, W), BF16),
        pltpu.VMEM((rows_m, L), BF16),
        pltpu.VMEM((rows_m, L), BF16),
        pltpu.VMEM((rows_m, L), BF16),
        pltpu.VMEM((2, n_ep, stride, L), BF16),
        pltpu.VMEM((n_ep, stride, L), BF16),
        pltpu.VMEM((2, rows_m, W), F32),
        pltpu.VMEM((2, rows_e, W), F32),
        dma((Z * (n_y // 2),)),
        dma((Z * (n_y // 2),)),
        dma((7,)),
        dma((Z,)),
        dma((5,)),
        dma((5,)),
        dma((5,)),
        dma((4,)),
        dma((8,)),
        pltpu.SemaphoreType.REGULAR((1,)),
        pltpu.VMEM((rows_m, 3 * W), F32),
    ]
    both = pl.pallas_call(
        functools.partial(kernel, n_ep, n_y, cap, stride),
        out_shape=pltpu.VMEM((mix_input.shape[0] + tok, L), BF16),
        in_specs=[any_spec] * 14,
        out_specs=vmem,
        scratch_shapes=scratch,
        compiler_params=pltpu.CompilerParams(
            collective_id=0, has_side_effects=True, vmem_limit_bytes=56 * 1024 * 1024
        ),
    )(
        mix_input,
        mix_gain.reshape(1, width),
        gate_b_weight,
        gate_c_weight,
        value_weight,
        conv_weight,
        out_weight,
        expert_input,
        expert_gain.reshape(1, width),
        routes.T,
        route_weight.T,
        jnp.swapaxes(expert_gate, 1, 2)[0],
        jnp.swapaxes(expert_up, 1, 2)[0],
        expert_down[0],
    )
    return pl.pallas_call(
        deliver,
        out_shape=(
            jax.ShapeDtypeStruct(mix_input.shape, BF16),
            jax.ShapeDtypeStruct(expert_input.shape, BF16),
        ),
        in_specs=[vmem],
        out_specs=(any_spec, any_spec),
        scratch_shapes=[dma((2,))],
    )(pltpu.with_memory_space_constraint(both, pltpu.VMEM))


def solution(mesh):
    in_specs = (
        P("ep", "tp"),
        P(),
        P(None, "tp"),
        P(None, "tp"),
        P(None, "tp"),
        P(None, "tp"),
        P("tp", None),
        P("ep", "tp"),
        P(),
        P("ep", None),
        P("ep", None),
        P("ep", None, "tp"),
        P("ep", None, "tp"),
        P("ep", "tp", None),
    )
    out_specs = (P("ep", "tp"), P("ep", "tp"))
    return jax.shard_map(local, mesh=mesh, in_specs=in_specs, out_specs=out_specs, check_vma=False)
```
